32 devices in a mesh: sp: 16 (over z, y, core), tp: 2 (over x).
Axes of the slice: x: 2, y: 2, z: 4, core: 2. Of those that a mesh axis runs over, the one named last changes fastest.
Arguments:
- query_content: bfloat16 [3072, 1024], P('sp'), may hold values from -6 to 6
- query_rotary: bfloat16 [3072, 512], P('sp'), may hold values from -8 to 8
- latents: bfloat16 [3072, 256], P(('sp', 'tp')), may hold values from -6 to 6
- key_rotary: bfloat16 [3072, 64], P(('sp', 'tp')), may hold values from -8 to 8
- latent_gain: float32 [256], replicated, may hold values from 0.1 to 1.9
- key_up: bfloat16 [256, 1024], P(None, 'tp'), may hold values from -0.375 to 0.375
- value_up: bfloat16 [256, 1024], P(None, 'tp'), may hold values from -0.375 to 0.375
- out_proj: bfloat16 [1024, 2048], P(None, 'tp'), may hold values from -2 to 2
- residual: bfloat16 [3072, 2048], P('sp', 'tp'), may hold values from -6 to 6
- mixer_gain: float32 [2048], replicated, may hold values from 0.1 to 1.9
- gate_proj: bfloat16 [2048, 5632], P('sp', 'tp'), may hold values from -0.125 to 0.125
- up_proj: bfloat16 [2048, 5632], P('sp', 'tp'), may hold values from -0.125 to 0.125
- down_proj: bfloat16 [5632, 2048], P('tp', 'sp'), may hold values from -0.078125 to 0.078125
Outputs:
- layer_out: bfloat16 [3072, 2048], P('sp', 'tp')
The draws below stay inside these ranges and needn't reach their ends.
All inputs are finite; a program needn't handle non-finite values.
Results may differ from the reference program's by a relative error of at most 0.011.
Values may be sent and summed in bfloat16 or wider, within the bound.
A program may use at most 128 MiB of HBM per device.

```python
import math
import jax
import jax.numpy as jnp
from jax import lax

D = 2048
H = 8
DN = 128
DR = 64
DV = 128
KVR = 256
FF = 5632
SPAN = 64
TOK = 192
SEQ = 3072
N_SP = 16
N_TP = 2


def draw_query_rotary(key, part):
    base = jax.random.normal(jax.random.fold_in(key, 14), (SEQ, H * DR), jnp.float32)
    return jnp.clip(base, -6.0, 6.0).astype(jnp.bfloat16)


def draw_key_rotary(key, part):
    base = jax.random.normal(jax.random.fold_in(key, 15), (SEQ, DR), jnp.float32)
    return jnp.clip(base, -6.0, 6.0).astype(jnp.bfloat16)


def shard_levels(own_key, dims, shards, least, high):
    level, own = 1.0, jax.random.fold_in(own_key, 6)
    for position, parts in shards:
        heights = jnp.exp(jax.random.uniform(jax.random.fold_in(own, position), (parts,), jnp.float32, least / len(shards), high / len(shards)))
        level = level * jnp.repeat(heights, dims[position] // parts).reshape([-1 if axis == position else 1 for axis in range(len(dims))])
    return level


def scatter_about(stream_key, shape, deviation, limit, pieces=(), kind=jnp.bfloat16):
    result = deviation * jax.random.normal(stream_key, shape, jnp.float32)
    if pieces:
        result = result * shard_levels(stream_key, shape, pieces, -0.22, 0.18)
    return jnp.clip(result, -limit, limit).astype(kind)


def setup_inputs(seed: int = 0) -> dict:
    key_of = jax.random.split(jax.random.key(seed), 14)
    query_content = scatter_about(key_of[0], (SEQ, H * DN), 1.0, 6.0, ((0, 16),))
    query_rotary = draw_query_rotary(jax.random.fold_in(key_of[13], 71), 0)
    latents = scatter_about(key_of[2], (SEQ, KVR), 1.0, 6.0, ((0, 32),))
    key_rotary = draw_key_rotary(jax.random.fold_in(key_of[13], 71), 0)
    latent_gain = jnp.clip(1.0 + 0.18 * jax.random.normal(key_of[4], (KVR,), jnp.float32), 0.1, 1.9)
    key_up = scatter_about(key_of[5], (KVR, H * DN), KVR ** -0.5, 0.375, ((1, 2),))
    value_up = scatter_about(key_of[6], (KVR, H * DV), KVR ** -0.5, 0.375, ((1, 2),))
    out_proj = scatter_about(key_of[7], (H * DV, D), (H * DV // 128) ** -0.5, 2.0, ((1, 2),))
    residual = scatter_about(key_of[8], (SEQ, D), 1.0, 6.0, ((0, 16), (1, 2)))
    mixer_gain = jnp.clip(1.0 + 0.18 * jax.random.normal(key_of[9], (D,), jnp.float32), 0.1, 1.9)
    gate_proj = scatter_about(key_of[10], (D, FF), D ** -0.5, 0.125, ((0, 16), (1, 2)))
    up_proj = scatter_about(key_of[11], (D, FF), D ** -0.5, 0.125, ((0, 16), (1, 2)))
    down_proj = scatter_about(key_of[12], (FF, D), FF ** -0.5, 0.078125, ((0, 2), (1, 16)))
    return {"query_content": query_content, "query_rotary": query_rotary, "latents": latents, "key_rotary": key_rotary, "latent_gain": latent_gain, "key_up": key_up, "value_up": value_up, "out_proj": out_proj, "residual": residual, "mixer_gain": mixer_gain, "gate_proj": gate_proj, "up_proj": up_proj, "down_proj": down_proj}


epsilon = 1e-06
masked_score = -1e+30

def norm_round(inputs, scales):
    widened = inputs.astype(jnp.float32)
    factor = lax.rsqrt(lax.optimization_barrier(jnp.mean(widened * widened, axis=-1, keepdims=True)) + epsilon)
    return (widened * factor * scales.astype(jnp.float32)).astype(jnp.bfloat16)

def rotate(inputs, places):
    dimension = inputs.shape[-1]
    middle = dimension // 2
    inverse = 10000.0 ** (-jnp.arange(0, dimension, 2, dtype=jnp.float32) / dimension)
    angles = places.astype(jnp.float32)[:, None, None] * inverse[None, None, :]
    cosine_table = jnp.cos(angles)
    sine_table = jnp.sin(angles)
    widened = inputs.astype(jnp.float32)
    first_half = widened[..., :middle]
    second_half = widened[..., middle:]
    return jnp.concatenate([first_half * cosine_table - second_half * sine_table, second_half * cosine_table + first_half * sine_table], axis=-1).astype(jnp.bfloat16)

def reference(query_content, query_rotary, latents, key_rotary, latent_gain, key_up, value_up, out_proj, residual, mixer_gain, gate_proj, up_proj, down_proj):
    per_device = TOK // N_TP
    normed = norm_round(latents, latent_gain)
    key_content = jnp.dot(normed, key_up, preferred_element_type=jnp.float32).astype(jnp.bfloat16)
    values = jnp.dot(normed, value_up, preferred_element_type=jnp.float32).astype(jnp.bfloat16)
    places = jnp.arange(SEQ, dtype=jnp.int32)
    key_turned = rotate(key_rotary[:, None, :], places)[:, 0, :]
    query_turned = rotate(query_rotary.reshape(SEQ, H, DR), places)
    key_content, values, key_turned, query_turned = lax.optimization_barrier((key_content, values, key_turned, query_turned))

    def subsets(inputs):
        shaped = inputs.reshape((N_SP, N_TP, per_device) + inputs.shape[1:])
        return jnp.swapaxes(shaped, 0, 1).reshape((N_TP, N_SP * per_device) + inputs.shape[1:])
    grouped = (subsets(key_content.reshape(SEQ, H, DN)), subsets(values.reshape(SEQ, H, DV)), subsets(key_turned), subsets(places))
    score_scale = 1.0 / math.sqrt(DN + DR)

    def one_block(query_block):
        contents, turned, query_places = query_block

        def one_subset(subset):
            key_rows, value_rows, key_turns, key_places = subset
            scores = (jnp.einsum('qhd,khd->qhk', contents.astype(jnp.float32), key_rows.astype(jnp.float32)) + jnp.einsum('qhr,kr->qhk', turned.astype(jnp.float32), key_turns.astype(jnp.float32))) * score_scale
            allowed = (key_places[None, :] // SPAN <= query_places[:, None] // SPAN)[:, None, :]
            highest = lax.optimization_barrier(jnp.max(jnp.where(allowed, scores, masked_score), axis=-1))
            weights = jnp.where(allowed, jnp.exp(scores - highest[..., None]), 0.0)
            weight_sum = lax.optimization_barrier(jnp.sum(weights, axis=-1))
            rounded = lax.optimization_barrier(weights.astype(jnp.bfloat16))
            weighted = jnp.einsum('qhk,khv->qhv', rounded.astype(jnp.float32), value_rows.astype(jnp.float32))
            return (highest, weight_sum, weighted)
        highest, weight_sum, weighted = lax.map(one_subset, grouped)
        overall = lax.optimization_barrier(jnp.max(highest, axis=0))
        factor = jnp.exp(highest - overall)
        merged = lax.optimization_barrier(jnp.sum(factor[..., None] * weighted, axis=0)) / lax.optimization_barrier(jnp.sum(factor * weight_sum, axis=0))[..., None]
        return merged.astype(jnp.bfloat16).reshape(TOK, H * DV)
    blocks = (query_content.reshape(N_SP, TOK, H, DN), query_turned.reshape(N_SP, TOK, H, DR), places.reshape(N_SP, TOK))
    head_out = lax.map(one_block, blocks).reshape(SEQ, H * DV)
    mixed_rows = (residual.astype(jnp.float32) + jnp.dot(head_out, out_proj, preferred_element_type=jnp.float32)).astype(jnp.bfloat16)
    mixed_rows = lax.optimization_barrier(mixed_rows)
    normed_rows = norm_round(mixed_rows, mixer_gain)
    hidden = (jax.nn.silu(jnp.dot(normed_rows, gate_proj, preferred_element_type=jnp.float32)) * jnp.dot(normed_rows, up_proj, preferred_element_type=jnp.float32)).astype(jnp.bfloat16)
    return (mixed_rows.astype(jnp.float32) + jnp.dot(hidden, down_proj, preferred_element_type=jnp.float32)).astype(jnp.bfloat16)
```

```python
import functools
import math

import jax
import jax.numpy as jnp
import numpy as np
from jax import lax
from jax.experimental import pallas as pl
from jax.experimental.pallas import tpu as pltpu
from jax.sharding import Mesh, PartitionSpec as P

H = 8
DN = 128
DR = 64
DV = 128
SPAN = 64


epsilon = 1e-06
masked_score = -1e30
SP = ("z", "y", "c")


def norm_round(inputs, scales):
    widened = inputs.astype(jnp.float32)
    factor = lax.rsqrt(jnp.mean(widened * widened, axis=-1, keepdims=True) + epsilon)
    return (widened * factor * scales).astype(jnp.bfloat16)


def rotate(inputs, places):
    dimension = inputs.shape[-1]
    middle = dimension // 2
    inverse = 10000.0 ** (-jnp.arange(0, dimension, 2, dtype=jnp.float32) / dimension)
    angles = places.astype(jnp.float32)[:, None, None] * inverse[None, None, :]
    cosine_table = jnp.cos(angles)
    sine_table = jnp.sin(angles)
    widened = inputs.astype(jnp.float32)
    first_half = widened[..., :middle]
    second_half = widened[..., middle:]
    return jnp.concatenate(
        [
            first_half * cosine_table - second_half * sine_table,
            second_half * cosine_table + first_half * sine_table,
        ],
        axis=-1,
    ).astype(jnp.bfloat16)


def hop(inputs, axis, offset):
    count = lax.axis_size(axis)
    return lax.ppermute(inputs, axis, [(i, (i + offset) % count) for i in range(count)])


def others(inputs, axis):
    return [inputs] + [hop(inputs, axis, d) for d in range(1, lax.axis_size(axis))]


def take(inputs, index, count, dim):
    size = inputs.shape[dim] // count
    return lax.dynamic_slice_in_dim(inputs, index * size, size, dim)


def in_order(blocks, axis, dim):
    count, me = lax.axis_size(axis), lax.axis_index(axis)
    if count == 1:
        return blocks[0]
    if count == 2:
        straight = jnp.concatenate(blocks, axis=dim)
        turned = jnp.concatenate(blocks[::-1], axis=dim)
        return jnp.where(me == 0, straight, turned)
    size = blocks[0].shape[dim]
    shape = list(blocks[0].shape)
    shape[dim] = size * count
    result = jnp.zeros(shape, blocks[0].dtype)
    for d, block in enumerate(blocks):
        place = lax.rem(me - d + count, count) * size
        result = lax.dynamic_update_slice_in_dim(result, block, place, dim)
    return result


def shards(
    query_content,
    query_rotary,
    latents,
    key_rotary,
    latent_gain,
    key_up,
    value_up,
    out_proj,
    residual,
    mixer_gain,
    gate_proj,
    up_proj,
    down_proj,
):
    query_rows = query_content.shape[0]
    tp_count, z_count = lax.axis_size("tp"), lax.axis_size("z")
    sp_index, tp_index, z_index = (
        lax.axis_index(SP),
        lax.axis_index("tp"),
        lax.axis_index("z"),
    )
    rank = latents.shape[1]
    per_device = latents.shape[0]
    heads = H // tp_count

    gathered = jnp.concatenate([latents, key_rotary], axis=1)
    places = (sp_index * tp_count + tp_index) * per_device + jnp.arange(
        per_device, dtype=jnp.int32
    )
    strides = {
        "z": lax.axis_size("y") * lax.axis_size("c") * tp_count * per_device,
        "y": lax.axis_size("c") * tp_count * per_device,
        "c": tp_count * per_device,
        "tp": per_device,
    }
    pieces = []
    for weights in (gate_proj, up_proj, down_proj.T):
        rows, columns = weights.shape
        pieces.append(jnp.swapaxes(weights.reshape(rows, z_count, columns // z_count), 0, 1))
    for axis in ("z", "tp", "y", "c"):
        count, me = lax.axis_size(axis), lax.axis_index(axis)
        gathered = jnp.concatenate(others(gathered, axis), axis=0)
        places = jnp.concatenate(
            [places + (lax.rem(me - d + count, count) - me) * strides[axis] for d in range(count)]
        )
        if axis == "z":
            gathered, pieces = lax.optimization_barrier((gathered, pieces))

    whole = []
    for piece in pieces:
        rows, units = piece.shape[1:]
        blocks = []
        for d in range(z_count):
            block = take(piece, lax.rem(z_index + d, z_count), z_count, 0)
            blocks.append(hop(block, "z", d) if d else block)
        block = in_order(blocks, "z", 0)[:, None]
        block = in_order(others(block, "y"), "y", 1)[:, :, None]
        block = in_order(others(block, "c"), "c", 2)
        whole.append(block.reshape(-1, units))
    gate, up, down = whole

    query_places = sp_index * query_rows + jnp.arange(query_rows, dtype=jnp.int32)
    normed = norm_round(gathered[:, :rank], latent_gain)
    key_turned = rotate(gathered[:, None, rank:], places)[:, 0, :]
    own_rotary = take(query_rotary, tp_index, tp_count, 1)
    own_content = take(query_content, tp_index, tp_count, 1)
    query_turned = rotate(own_rotary.reshape(query_rows, heads, DR), query_places)
    allowed = places[None, :] // SPAN <= query_places[:, None] // SPAN
    score_scale = 1.0 / math.sqrt(DN + DR)
    key_rows = jnp.dot(normed, key_up, preferred_element_type=jnp.float32).astype(jnp.bfloat16)
    value_rows = jnp.dot(normed, value_up, preferred_element_type=jnp.float32).astype(jnp.bfloat16)
    outs = []
    for h in range(heads):
        k = jnp.concatenate([key_rows[:, h * DN : (h + 1) * DN], key_turned], axis=1)
        q = jnp.concatenate(
            [own_content[:, h * DN : (h + 1) * DN], query_turned[:, h, :]], axis=1
        )
        scores = lax.dot_general(
            q, k, (((1,), (1,)), ((), ())), preferred_element_type=jnp.float32
        )
        scores = jnp.where(allowed, scores * score_scale, masked_score)
        highest = jnp.max(scores, axis=-1, keepdims=True)
        weights = jnp.where(allowed, jnp.exp(scores - highest), 0.0)
        weight_sum = jnp.sum(weights, axis=-1, keepdims=True)
        weighted = jnp.dot(
            weights.astype(jnp.bfloat16),
            value_rows[:, h * DV : (h + 1) * DV],
            preferred_element_type=jnp.float32,
        )
        outs.append((weighted / weight_sum).astype(jnp.bfloat16))
    own_heads = jnp.concatenate(outs, axis=1)
    total = residual.astype(jnp.float32)
    for d, block in enumerate(others(own_heads, "tp")):
        part = take(out_proj, lax.rem(tp_index - d + tp_count, tp_count), tp_count, 0)
        total = total + jnp.dot(block, part, preferred_element_type=jnp.float32)
    mixed_rows = total.astype(jnp.bfloat16)

    result = mixed_rows.astype(jnp.float32)
    for d, rows in enumerate(others(mixed_rows, "z")):
        normed_rows = norm_round(in_order(others(rows, "tp"), "tp", 1), mixer_gain)
        hidden = (
            jax.nn.silu(jnp.dot(normed_rows, gate, preferred_element_type=jnp.float32))
            * jnp.dot(normed_rows, up, preferred_element_type=jnp.float32)
        ).astype(jnp.bfloat16)

        def share(index):
            part = take(down, lax.rem(index, tp_count), tp_count, 0)
            return lax.dot_general(
                hidden, part, (((1,), (1,)), ((), ())), preferred_element_type=jnp.float32
            )

        arrived = [
            hop(share(tp_index + e).astype(jnp.bfloat16), "tp", e) for e in range(1, tp_count)
        ]
        sums = share(tp_index)
        for part in arrived:
            sums = sums + part.astype(jnp.float32)
        if d:
            sums = hop(sums.astype(jnp.bfloat16), "z", -d).astype(jnp.float32)
        result = result + sums
    return result.astype(jnp.bfloat16)


Y, C, X = 2, 2, 2
LANES = 128
MESH = pl.DeviceIdType.MESH
VMEM = pltpu.VMEM
F32, BF16 = jnp.float32, jnp.bfloat16


def nearest(z_count):
    return [
        sorted(range(z_count), key=lambda s: (abs(s - z), s)) for z in range(z_count)
    ]


def pick(index, values):
    result = jnp.int32(values[0])
    for k in range(1, len(values)):
        result = jnp.where(index == k, jnp.int32(values[k]), result)
    return result


def split_blocks(blocks, z_count):
    least, left = divmod(blocks, z_count)
    low, high = left - left // 2, left // 2
    return least, low, z_count - high


def rotary_tables(positions):
    inverse = np.float32(10000.0) ** (-np.arange(0, DR, 2, dtype=np.float32) / np.float32(DR))
    angles = positions.astype(np.float32)[:, None] * inverse.astype(np.float32)[None, :]
    wide = angles.astype(np.float64)
    repeat = LANES // (DR // 2)
    return (
        np.tile(np.cos(wide).astype(np.float32), (1, repeat)),
        np.tile(np.sin(wide).astype(np.float32), (1, repeat)),
    )


def turn_matrices():
    middle = DR // 2
    turn = np.zeros((DR, DR), np.float32)
    for i in range(middle):
        turn[middle + i, i] = -1.0
        turn[i, middle + i] = 1.0
    copies = LANES // DR
    same = np.concatenate([np.eye(DR, dtype=np.float32)] * copies, axis=1)
    turned = np.concatenate([turn] * copies, axis=1)
    paired = np.kron(np.eye(copies, dtype=np.float32), turn)
    return same, turned, paired


def layer_kernel(
    z_count,
    qc_ref,
    qr_ref,
    lat_ref,
    kr_ref,
    lgain_ref,
    key_up_ref,
    value_up_ref,
    mgain_ref,
    same_ref,
    turned_ref,
    paired_ref,
    oproj_hbm,
    res_hbm,
    gate_hbm,
    up_hbm,
    down_hbm,
    cos_hbm,
    sin_hbm,
    out_ref,
    lat_buf,
    kr_buf,
    cos_buf,
    sin_buf,
    oproj_buf,
    res_buf,
    gate_buf,
    up_buf,
    down_buf,
    key_s,
    value_s,
    turn_s,
    q_s,
    max_s,
    sum_s,
    acc_s,
    ho_buf,
    tok_buf,
    nrm_s,
    hid_s,
    own_s,
    fin_s,
    xs_send,
    xs_recv,
    zs_send,
    zs_recv,
    loc_sem,
    lz_s,
    lz_r,
    ly_s,
    ly_r,
    lx_s,
    lx_r,
    lc_s,
    lc_r,
    wz_s,
    wz_r,
    wy_s,
    wy_r,
    wc_s,
    wc_r,
    ho_sem,
    tu_s,
    td_s,
    tz_r,
    tx_s,
    tx_r,
    rx_s,
    rx_r,
    rz_s,
    rz_r,
):
    sp, x = lax.axis_index("sp"), lax.axis_index("tp")
    z, y, c = sp // (Y * C), (sp // C) % Y, sp % C
    order = nearest(z_count)
    rows = qc_ref.shape[0]
    per_device = lat_ref.shape[0]
    rank = lat_ref.shape[1]
    chunk = Y * C * X * per_device
    heads = key_up_ref.shape[1] // DN
    depth = gate_hbm.shape[0]
    blocks = gate_hbm.shape[1] // LANES
    least, low, high = split_blocks(blocks, z_count)
    main = least * LANES
    half = res_hbm.shape[1]

    def dev(zz, yy, cc, xx):
        return ((zz * Y + yy) * C + cc, xx)

    def has_extra(zz):
        return (zz < low) | (zz >= high)

    def offset(zz):
        return (zz * least + jnp.minimum(zz, low) + jnp.maximum(zz - high, 0)) * LANES

    def remote(src, dst, send, recv, to):
        return pltpu.make_async_remote_copy(
            src_ref=src,
            dst_ref=dst,
            send_sem=send,
            recv_sem=recv,
            device_id=to,
            device_id_type=MESH,
        )

    y_peer, x_peer, c_peer = dev(z, 1 - y, c, x), dev(z, y, c, 1 - x), dev(z, y, 1 - c, x)

    slot = sp
    own = offset(z)

    def weight_block(m, index, extra):
        if m < 2:
            buf = (gate_buf, up_buf)[m]
            lanes = pl.ds(main, LANES) if extra else pl.ds(0, main)
            return buf.at[pl.ds(pl.multiple_of(index * depth, depth), depth), lanes]
        lines = pl.ds(main, LANES) if extra else pl.ds(0, main)
        return down_buf.at[index, lines]

    def weight_source(m, zz, extra):
        start = pl.multiple_of(offset(zz) + (main if extra else 0), LANES)
        size = LANES if extra else main
        if m < 2:
            return (gate_hbm, up_hbm)[m].at[:, pl.ds(start, size)]
        return down_hbm.at[pl.ds(start, size)]

    locals_ = [
        (lat_ref, lat_buf.at[z, c, y, x], 0),
        (kr_ref, kr_buf.at[z, c, y, x], 1),
        (cos_hbm, cos_buf, 2),
        (sin_hbm, sin_buf, 3),
        (oproj_hbm, oproj_buf, 4),
        (res_hbm, res_buf, 5),
    ]

    def local(k):
        src, dst, sem = locals_[k]
        return pltpu.make_async_copy(src, dst, loc_sem.at[sem])

    def own_weight(m, extra):
        return pltpu.make_async_copy(
            weight_source(m, z, extra),
            weight_block(m, slot, extra),
            loc_sem.at[6 + 2 * m + int(extra)],
        )

    for k in range(len(locals_)):
        local(k).start()
    for m in range(3):
        own_weight(m, False).start()

    @pl.when(has_extra(z))
    def _():
        for m in range(3):
            own_weight(m, True).start()

    @pl.when(jnp.logical_not(has_extra(z)))
    def _():
        gate_buf[:, main:] = jnp.zeros((gate_buf.shape[0], LANES), BF16)
        up_buf[:, main:] = jnp.zeros((up_buf.shape[0], LANES), BF16)
        down_buf[:, main:, :] = jnp.zeros((down_buf.shape[0], LANES, LANES), BF16)

    barrier = pltpu.get_barrier_semaphore()
    for peer in (y_peer, x_peer, c_peer):
        pl.semaphore_signal(barrier, inc=1, device_id=peer, device_id_type=MESH)
    for d in range(1, z_count):
        pl.semaphore_signal(
            barrier,
            inc=1,
            device_id=dev(lax.rem(z + d, z_count), y, c, x),
            device_id_type=MESH,
        )
    pl.semaphore_wait(barrier, 3 + z_count - 1)

    lats = ((lat_ref, lat_buf), (kr_ref, kr_buf))

    def lat_z(p, source, target):
        return remote(
            lats[p][0],
            lats[p][1].at[source, c, y, x],
            lz_s.at[target, p],
            lz_r.at[source, p],
            dev(target, y, c, x),
        )

    def lat_y(p, zz):
        block = lats[p][1].at[zz, c, y, x]
        return remote(block, block, ly_s.at[zz, p], ly_r.at[zz, p], y_peer)

    def lat_y_in(p, zz):
        block = lats[p][1].at[zz, c, 1 - y, x]
        return remote(block, block, ly_s.at[zz, p], ly_r.at[zz, p], y_peer)

    def lat_x(p, zz, xx):
        block = lats[p][1].at[zz, c, :, xx]
        return remote(block, block, lx_s.at[zz, p], lx_r.at[zz, p], x_peer)

    def lat_c(p, zz, cc):
        block = lats[p][1].at[zz, cc]
        return remote(block, block, lc_s.at[zz, p], lc_r.at[zz, p], c_peer)

    for p in range(2):
        local(p).wait()
    for p in range(2):
        lat_y(p, z).start()
    for d in range(1, z_count):

        @pl.when(z + d < z_count)
        def _():
            for p in range(2):
                lat_z(p, z, z + d).start()

    def weight_z(m, source, target, extra, index):
        return remote(
            weight_source(m, target, extra),
            weight_block(m, index, extra),
            wz_s.at[target, m, int(extra)],
            wz_r.at[source, m, int(extra)],
            dev(target, y, c, x),
        )

    def each_part(zz, action):
        action(False)

        @pl.when(has_extra(zz))
        def _():
            action(True)

    for s in range(1, z_count):
        target = pick(z, [o[s] for o in order])
        for m in range(3):
            each_part(target, lambda e: weight_z(m, z, target, e, slot).start())

    for p in range(2):
        lat_y_in(p, z).wait_recv()
        lat_x(p, z, x).start()

    def lower(action):
        for d in range(1, z_count):

            @pl.when(z >= d)
            def _():
                for p in range(2):
                    action(p, z - d)

    def y_step(p, zz):
        lat_z(p, zz, z).wait_recv()
        lat_y(p, zz).start()

    lower(y_step)
    for p in range(2):
        lat_x(p, z, 1 - x).wait_recv()
        lat_c(p, z, c).start()

    def x_step(p, zz):
        lat_y_in(p, zz).wait_recv()
        lat_x(p, zz, x).start()

    lower(x_step)

    def block_of(zz, yy, cc):
        return (zz * Y + yy) * C + cc

    def weight_y(m, zz, yy, extra):
        block = weight_block(m, block_of(zz, yy, c), extra)
        return remote(
            block, block, wy_s.at[zz, m, int(extra)], wy_r.at[zz, m, int(extra)], y_peer
        )

    def weight_c(m, zz, yy, cc, extra):
        block = weight_block(m, block_of(zz, yy, cc), extra)
        return remote(
            block,
            block,
            wc_s.at[zz, yy, m, int(extra)],
            wc_r.at[zz, yy, m, int(extra)],
            c_peer,
        )

    for m in range(3):
        each_part(z, lambda e: own_weight(m, e).wait())
        each_part(z, lambda e: weight_y(m, z, y, e).start())
        each_part(z, lambda e: weight_c(m, z, y, c, e).start())

    def c_step(p, zz):
        lat_x(p, zz, 1 - x).wait_recv()
        lat_c(p, zz, c).start()

    lower(c_step)

    local(2).wait()
    local(3).wait()
    q_start = pl.multiple_of((c * Y + y) * rows, rows)
    cos_q = cos_buf[z, pl.ds(q_start, rows), :]
    sin_q = sin_buf[z, pl.ds(q_start, rows), :]
    lane = lax.broadcasted_iota(jnp.int32, (rows, LANES), 1)
    for pair in range(heads * DR // LANES):
        start = pl.multiple_of(x * heads * DR + pair * LANES, LANES)
        part = qr_ref[:, pl.ds(start, LANES)]
        swapped = jnp.dot(part, paired_ref[...], preferred_element_type=F32)
        turned = (part.astype(F32) * cos_q + swapped * sin_q).astype(BF16)
        for k in range(LANES // DR):
            h = pair * (LANES // DR) + k
            keep = (lane >= k * DR) & (lane < (k + 1) * DR)
            q_s[h, :, LANES:] = jnp.where(keep, turned, jnp.zeros_like(turned))
    for h in range(heads):
        start = pl.multiple_of(x * heads * DN + h * DN, DN)
        q_s[h, :, :LANES] = qc_ref[:, pl.ds(start, DN)]

    scale = 1.0 / math.sqrt(DN + DR)
    max_s[...] = jnp.full(max_s.shape, masked_score, F32)
    sum_s[...] = jnp.zeros(sum_s.shape, F32)
    acc_s[...] = jnp.zeros(acc_s.shape, F32)
    key_id = lax.broadcasted_iota(jnp.int32, (rows, chunk), 1)
    per_c, per_y = Y * X * per_device, X * per_device
    c_id = key_id // per_c
    y_id = (key_id // per_y) % Y
    key_place = y_id * C * per_y + c_id * per_y + key_id % per_y
    query_place = (y * C + c) * per_y + lax.broadcasted_iota(jnp.int32, (rows, chunk), 0)

    def attend(d, carry):
        zz = z - d
        for p in range(2):
            lat_c(p, zz, 1 - c).wait_recv()
        wide = lat_buf[zz].reshape(chunk, rank).astype(F32)
        factor = lax.rsqrt(jnp.mean(wide * wide, axis=-1, keepdims=True) + epsilon)
        normed = (wide * factor * lgain_ref[...]).astype(BF16)
        key_s[...] = jnp.dot(normed, key_up_ref[...], preferred_element_type=F32).astype(BF16)
        value_s[...] = jnp.dot(normed, value_up_ref[...], preferred_element_type=F32).astype(BF16)
        rot = kr_buf[zz].reshape(chunk, DR)
        straight = jnp.dot(rot, same_ref[...], preferred_element_type=F32)
        swapped = jnp.dot(rot, turned_ref[...], preferred_element_type=F32)
        turn_s[...] = (straight * cos_buf[zz] + swapped * sin_buf[zz]).astype(BF16)
        allowed = (key_place - d * chunk) // SPAN <= query_place // SPAN
        for h in range(heads):
            k = jnp.concatenate([key_s[:, h * DN : (h + 1) * DN], turn_s[...]], axis=1)
            scores = lax.dot_general(
                q_s[h], k, (((1,), (1,)), ((), ())), preferred_element_type=F32
            )
            scores = jnp.where(allowed, scores * scale, masked_score)
            before = max_s[h, :, :1]
            peak = jnp.maximum(before, jnp.max(scores, axis=-1, keepdims=True))
            weights = jnp.exp(scores - peak)
            fade = jnp.exp(before - peak)
            total = sum_s[h, :, :1] * fade + jnp.sum(weights, axis=-1, keepdims=True)
            gained = jnp.dot(
                weights.astype(BF16),
                value_s[:, h * DV : (h + 1) * DV],
                preferred_element_type=F32,
            )
            acc_s[h] = acc_s[h] * fade + gained
            max_s[h] = jnp.broadcast_to(peak, max_s.shape[1:])
            sum_s[h] = jnp.broadcast_to(total, sum_s.shape[1:])
        return carry

    lax.fori_loop(0, z + 1, attend, 0)
    for h in range(heads):
        ho_buf[x, :, h * DV : (h + 1) * DV] = (acc_s[h] / sum_s[h]).astype(BF16)

    def heads_out(xx):
        return remote(ho_buf.at[xx], ho_buf.at[xx], ho_sem.at[0], ho_sem.at[1], x_peer)

    heads_out(x).start()

    def relay_y(s):
        zz = pick(z, [o[s] for o in order])
        for m in range(3):
            each_part(z, lambda e: weight_z(m, zz, z, e, block_of(zz, y, c)).wait_recv())
            each_part(z, lambda e: weight_y(m, zz, y, e).start())
            each_part(z, lambda e: weight_c(m, zz, y, c, e).start())

    def relay_c(s):
        zz = pick(z, [o[s] for o in order])
        for m in range(3):
            each_part(z, lambda e: weight_y(m, zz, 1 - y, e).wait_recv())
            each_part(z, lambda e: weight_c(m, zz, 1 - y, c, e).start())

    local(4).wait()
    local(5).wait()
    width = heads * DV
    heads_out(1 - x).wait_recv()
    total = res_buf[...].astype(F32)
    for k in range(X):
        total = total + jnp.dot(
            ho_buf[k], oproj_buf[k * width : (k + 1) * width, :], preferred_element_type=F32
        )
    tok_buf[z, x] = total.astype(BF16)

    def tok_z(zz, to, sem):
        block = tok_buf.at[zz, x]
        return remote(block, block, sem.at[zz], tz_r.at[zz], dev(to, y, c, x))

    def tok_x(zz, xx):
        block = tok_buf.at[zz, xx]
        return remote(block, block, tx_s.at[zz], tx_r.at[zz], x_peer)

    def goes_up(zz):
        return (zz <= z) & (z + 1 < z_count)

    def goes_down(zz):
        return (zz >= z) & (z > 0)

    def forward(zz):
        tok_x(zz, x).start()

        @pl.when(goes_up(zz))
        def _():
            tok_z(zz, z + 1, tu_s).start()

        @pl.when(goes_down(zz))
        def _():
            tok_z(zz, z - 1, td_s).start()

    forward(z)
    relay_y(1)
    relay_c(0)
    for s in range(2, z_count):
        relay_y(s)
        relay_c(s - 1)
    relay_c(z_count - 1)

    def relay_tokens(s):
        zz = pick(z, [o[s] for o in order])
        tok_z(zz, z, tu_s).wait_recv()
        forward(zz)

    relay_tokens(1)

    for s in range(z_count):
        zz = pick(z, [o[s] for o in order])
        for yy in range(Y):
            for m in range(3):
                each_part(z, lambda e: weight_c(m, zz, yy, 1 - c, e).wait_recv())

    pad = gate_buf.shape[1]
    wide_tile = 2 * LANES
    blocks_half = half // LANES

    def to_sum(zz):
        return remote(xs_send.at[zz], xs_recv.at[zz], rx_s.at[zz], rx_r.at[zz], x_peer)

    def mix(s):
        zz = pick(z, [o[s] for o in order])
        tok_x(zz, 1 - x).wait_recv()
        parts = [tok_buf[zz, k].astype(F32) for k in range(X)]
        squares = sum(jnp.sum(v * v, axis=-1, keepdims=True) for v in parts)
        factor = lax.rsqrt(squares / (X * half) + epsilon)
        for k in range(X):
            cut = slice(k * half, (k + 1) * half)
            nrm_s[:, cut] = (parts[k] * factor * mgain_ref[:, cut]).astype(BF16)

        def hidden(n, carry):
            lanes = pl.ds(pl.multiple_of(n * wide_tile, wide_tile), wide_tile)
            g = jnp.dot(nrm_s[...], gate_buf[:, lanes], preferred_element_type=F32)
            u = jnp.dot(nrm_s[...], up_buf[:, lanes], preferred_element_type=F32)
            hid_s[:, lanes] = (g / (1.0 + jnp.exp(-g)) * u).astype(BF16)
            return carry

        lax.fori_loop(0, pad // wide_tile, hidden, 0)

        def product(xx, n):
            first = xx * blocks_half + 2 * n
            w = jnp.concatenate([down_buf[first], down_buf[first + 1]], axis=1)
            return jnp.dot(hid_s[...], w, preferred_element_type=F32)

        def theirs(n, carry):
            lanes = pl.ds(pl.multiple_of(n * wide_tile, wide_tile), wide_tile)
            xs_send[zz, :, lanes] = product(1 - x, n).astype(BF16)
            return carry

        def ours(n, carry):
            lanes = pl.ds(pl.multiple_of(n * wide_tile, wide_tile), wide_tile)
            own_s[zz, :, lanes] = product(x, n)
            return carry

        lax.fori_loop(0, half // wide_tile, theirs, 0)
        to_sum(zz).start()
        lax.fori_loop(0, half // wide_tile, ours, 0)

    def to_owner(source, target):
        return remote(
            zs_send.at[target],
            zs_recv.at[source],
            rz_s.at[target],
            rz_r.at[source],
            dev(target, y, c, x),
        )

    def gather_sum(s):
        zz = pick(z, [o[s] for o in order])
        to_sum(zz).wait_recv()
        both = own_s[zz] + xs_recv[zz].astype(F32)
        if s == 0:
            fin_s[...] = both + tok_buf[z, x].astype(F32)
        else:
            zs_send[zz] = both.astype(BF16)
            to_owner(z, zz).start()

    for s in range(z_count):
        mix(s)
        if s + 2 < z_count:
            relay_tokens(s + 2)
        if s:
            gather_sum(s - 1)
    gather_sum(z_count - 1)
    result = fin_s[...]
    for s in range(1, z_count):
        zz = pick(z, [o[s] for o in order])
        to_owner(zz, z).wait_recv()
        result = result + zs_recv[zz].astype(F32)
    out_ref[...] = result.astype(out_ref.dtype)

    for p in range(2):
        lat_y(p, z).wait_send()
        lat_x(p, z, x).wait_send()
        lat_c(p, z, c).wait_send()
    for d in range(1, z_count):

        @pl.when(z + d < z_count)
        def _():
            for p in range(2):
                lat_z(p, z, z + d).wait_send()

    def lat_done(p, zz):
        lat_y(p, zz).wait_send()
        lat_x(p, zz, x).wait_send()
        lat_c(p, zz, c).wait_send()

    lower(lat_done)
    heads_out(x).wait_send()
    for s in range(z_count):
        zz = pick(z, [o[s] for o in order])
        for m in range(3):
            if s:
                each_part(zz, lambda e: weight_z(m, z, zz, e, slot).wait_send())
            each_part(z, lambda e: weight_y(m, zz, y, e).wait_send())
            each_part(z, lambda e: weight_c(m, zz, y, c, e).wait_send())
            each_part(z, lambda e: weight_c(m, zz, 1 - y, c, e).wait_send())
        tok_x(zz, x).wait_send()

        @pl.when(goes_up(zz))
        def _():
            tok_z(zz, z + 1, tu_s).wait_send()

        @pl.when(goes_down(zz))
        def _():
            tok_z(zz, z - 1, td_s).wait_send()

        to_sum(zz).wait_send()
        if s:
            to_owner(z, zz).wait_send()


def fits(mesh):
    return mesh.shape["tp"] == X and mesh.shape["sp"] % (2 * Y * C) == 0


def fused(mesh):
    sp_count = mesh.shape["sp"]
    z_count = sp_count // (Y * C)

    def shard(
        query_content,
        query_rotary,
        latents,
        key_rotary,
        latent_gain,
        key_up,
        value_up,
        out_proj,
        residual,
        mixer_gain,
        gate_proj,
        up_proj,
        down_proj,
    ):
        rows = query_content.shape[0]
        per_device, rank = latents.shape
        chunk = Y * C * X * per_device
        heads = key_up.shape[1] // DN
        half = residual.shape[1]
        depth, units = gate_proj.shape
        least, low, high = split_blocks(units // LANES, z_count)
        pad = (least + 2 - least % 2) * LANES
        model = X * half
        places = np.arange(z_count * chunk).reshape(z_count, Y, C, rows)
        places = places.transpose(0, 2, 1, 3).reshape(-1)
        cosines, sines = (t.reshape(z_count, chunk, LANES) for t in rotary_tables(places))
        same, turned, paired = (jnp.asarray(t, BF16) for t in turn_matrices())
        vmem = pl.BlockSpec(memory_space=VMEM)
        hbm = pl.BlockSpec(memory_space=pl.ANY)
        dma = pltpu.SemaphoreType.DMA
        scratch = [
            VMEM((z_count, C, Y, X, per_device, rank), BF16),
            VMEM((z_count, C, Y, X, per_device, DR), BF16),
            VMEM((z_count, chunk, LANES), F32),
            VMEM((z_count, chunk, LANES), F32),
            VMEM(out_proj.shape, BF16),
            VMEM((rows, half), BF16),
            VMEM((model, pad), BF16),
            VMEM((model, pad), BF16),
            VMEM((sp_count, pad, LANES), BF16),
            VMEM((chunk, heads * DN), BF16),
            VMEM((chunk, heads * DV), BF16),
            VMEM((chunk, LANES), BF16),
            VMEM((heads, rows, 2 * LANES), BF16),
            VMEM((heads, rows, LANES), F32),
            VMEM((heads, rows, LANES), F32),
            VMEM((heads, rows, DV), F32),
            VMEM((X, rows, heads * DV), BF16),
            VMEM((z_count, X, rows, half), BF16),
            VMEM((rows, model), BF16),
            VMEM((rows, pad), BF16),
            VMEM((z_count, rows, half), F32),
            VMEM((rows, half), F32),
            VMEM((z_count, rows, half), BF16),
            VMEM((z_count, rows, half), BF16),
            VMEM((z_count, rows, half), BF16),
            VMEM((z_count, rows, half), BF16),
            dma((12,)),
            *[dma((z_count, 2)) for _ in range(8)],
            *[dma((z_count, 3, 2)) for _ in range(4)],
            *[dma((z_count, Y, 3, 2)) for _ in range(2)],
            dma((2,)),
            *[dma((z_count,)) for _ in range(9)],
        ]
        return pl.pallas_call(
            functools.partial(layer_kernel, z_count),
            out_shape=jax.ShapeDtypeStruct(residual.shape, residual.dtype),
            in_specs=[vmem] * 11 + [hbm] * 7,
            out_specs=vmem,
            scratch_shapes=scratch,
            compiler_params=pltpu.CompilerParams(
                collective_id=0, has_side_effects=True, vmem_limit_bytes=60 * 1024 * 1024
            ),
        )(
            query_content,
            query_rotary,
            latents,
            key_rotary,
            latent_gain[None, :],
            key_up,
            value_up,
            mixer_gain[None, :],
            same,
            turned,
            paired,
            out_proj,
            residual,
            gate_proj,
            up_proj,
            down_proj,
            cosines,
            sines,
        )

    return jax.shard_map(
        shard,
        mesh=mesh,
        in_specs=(
            P("sp", None),
            P("sp", None),
            P(("sp", "tp"), None),
            P(("sp", "tp"), None),
            P(),
            P(None, "tp"),
            P(None, "tp"),
            P(None, "tp"),
            P("sp", "tp"),
            P(),
            P("sp", "tp"),
            P("sp", "tp"),
            P("tp", "sp"),
        ),
        out_specs=P("sp", "tp"),
        check_vma=False,
    )


def plain(mesh):
    sp_count, tp_count = mesh.shape["sp"], mesh.shape["tp"]
    grouped = Mesh(mesh.devices.reshape(sp_count // 4, 2, 2, tp_count), SP + ("tp",))
    return jax.shard_map(
        shards,
        mesh=grouped,
        in_specs=(
            P(SP, None),
            P(SP, None),
            P(SP + ("tp",), None),
            P(SP + ("tp",), None),
            P(),
            P(None, "tp"),
            P(None, "tp"),
            P(None, "tp"),
            P(SP, "tp"),
            P(),
            P(SP, "tp"),
            P(SP, "tp"),
            P("tp", SP),
        ),
        out_specs=P(SP, "tp"),
        check_vma=False,
    )


def solution(mesh):
    if fits(mesh):
        return fused(mesh)
    return plain(mesh)
```

```python
import functools
import math

import jax
import jax.numpy as jnp
import numpy as np
from jax import lax
from jax.experimental import pallas as pl
from jax.experimental.pallas import tpu as pltpu
from jax.sharding import Mesh, PartitionSpec as P

H = 8
DN = 128
DR = 64
DV = 128
SPAN = 64


epsilon = 1e-06
masked_score = -1e30
SP = ("z", "y", "c")


def norm_round(inputs, scales):
    widened = inputs.astype(jnp.float32)
    factor = lax.rsqrt(jnp.mean(widened * widened, axis=-1, keepdims=True) + epsilon)
    return (widened * factor * scales).astype(jnp.bfloat16)


def rotate(inputs, places):
    dimension = inputs.shape[-1]
    middle = dimension // 2
    inverse = 10000.0 ** (-jnp.arange(0, dimension, 2, dtype=jnp.float32) / dimension)
    angles = places.astype(jnp.float32)[:, None, None] * inverse[None, None, :]
    cosine_table = jnp.cos(angles)
    sine_table = jnp.sin(angles)
    widened = inputs.astype(jnp.float32)
    first_half = widened[..., :middle]
    second_half = widened[..., middle:]
    return jnp.concatenate(
        [
            first_half * cosine_table - second_half * sine_table,
            second_half * cosine_table + first_half * sine_table,
        ],
        axis=-1,
    ).astype(jnp.bfloat16)


def hop(inputs, axis, offset):
    count = lax.axis_size(axis)
    return lax.ppermute(inputs, axis, [(i, (i + offset) % count) for i in range(count)])


def others(inputs, axis):
    return [inputs] + [hop(inputs, axis, d) for d in range(1, lax.axis_size(axis))]


def take(inputs, index, count, dim):
    size = inputs.shape[dim] // count
    return lax.dynamic_slice_in_dim(inputs, index * size, size, dim)


def in_order(blocks, axis, dim):
    count, me = lax.axis_size(axis), lax.axis_index(axis)
    if count == 1:
        return blocks[0]
    if count == 2:
        straight = jnp.concatenate(blocks, axis=dim)
        turned = jnp.concatenate(blocks[::-1], axis=dim)
        return jnp.where(me == 0, straight, turned)
    size = blocks[0].shape[dim]
    shape = list(blocks[0].shape)
    shape[dim] = size * count
    result = jnp.zeros(shape, blocks[0].dtype)
    for d, block in enumerate(blocks):
        place = lax.rem(me - d + count, count) * size
        result = lax.dynamic_update_slice_in_dim(result, block, place, dim)
    return result


def shards(
    query_content,
    query_rotary,
    latents,
    key_rotary,
    latent_gain,
    key_up,
    value_up,
    out_proj,
    residual,
    mixer_gain,
    gate_proj,
    up_proj,
    down_proj,
):
    query_rows = query_content.shape[0]
    tp_count, z_count = lax.axis_size("tp"), lax.axis_size("z")
    sp_index, tp_index, z_index = (
        lax.axis_index(SP),
        lax.axis_index("tp"),
        lax.axis_index("z"),
    )
    rank = latents.shape[1]
    per_device = latents.shape[0]
    heads = H // tp_count

    gathered = jnp.concatenate([latents, key_rotary], axis=1)
    places = (sp_index * tp_count + tp_index) * per_device + jnp.arange(
        per_device, dtype=jnp.int32
    )
    strides = {
        "z": lax.axis_size("y") * lax.axis_size("c") * tp_count * per_device,
        "y": lax.axis_size("c") * tp_count * per_device,
        "c": tp_count * per_device,
        "tp": per_device,
    }
    pieces = []
    for weights in (gate_proj, up_proj, down_proj.T):
        rows, columns = weights.shape
        pieces.append(jnp.swapaxes(weights.reshape(rows, z_count, columns // z_count), 0, 1))
    for axis in ("z", "tp", "y", "c"):
        count, me = lax.axis_size(axis), lax.axis_index(axis)
        gathered = jnp.concatenate(others(gathered, axis), axis=0)
        places = jnp.concatenate(
            [places + (lax.rem(me - d + count, count) - me) * strides[axis] for d in range(count)]
        )
        if axis == "z":
            gathered, pieces = lax.optimization_barrier((gathered, pieces))

    whole = []
    for piece in pieces:
        rows, units = piece.shape[1:]
        blocks = []
        for d in range(z_count):
            block = take(piece, lax.rem(z_index + d, z_count), z_count, 0)
            blocks.append(hop(block, "z", d) if d else block)
        block = in_order(blocks, "z", 0)[:, None]
        block = in_order(others(block, "y"), "y", 1)[:, :, None]
        block = in_order(others(block, "c"), "c", 2)
        whole.append(block.reshape(-1, units))
    gate, up, down = whole

    query_places = sp_index * query_rows + jnp.arange(query_rows, dtype=jnp.int32)
    normed = norm_round(gathered[:, :rank], latent_gain)
    key_turned = rotate(gathered[:, None, rank:], places)[:, 0, :]
    own_rotary = take(query_rotary, tp_index, tp_count, 1)
    own_content = take(query_content, tp_index, tp_count, 1)
    query_turned = rotate(own_rotary.reshape(query_rows, heads, DR), query_places)
    allowed = places[None, :] // SPAN <= query_places[:, None] // SPAN
    score_scale = 1.0 / math.sqrt(DN + DR)
    key_rows = jnp.dot(normed, key_up, preferred_element_type=jnp.float32).astype(jnp.bfloat16)
    value_rows = jnp.dot(normed, value_up, preferred_element_type=jnp.float32).astype(jnp.bfloat16)
    outs = []
    for h in range(heads):
        k = jnp.concatenate([key_rows[:, h * DN : (h + 1) * DN], key_turned], axis=1)
        q = jnp.concatenate(
            [own_content[:, h * DN : (h + 1) * DN], query_turned[:, h, :]], axis=1
        )
        scores = lax.dot_general(
            q, k, (((1,), (1,)), ((), ())), preferred_element_type=jnp.float32
        )
        scores = jnp.where(allowed, scores * score_scale, masked_score)
        highest = jnp.max(scores, axis=-1, keepdims=True)
        weights = jnp.where(allowed, jnp.exp(scores - highest), 0.0)
        weight_sum = jnp.sum(weights, axis=-1, keepdims=True)
        weighted = jnp.dot(
            weights.astype(jnp.bfloat16),
            value_rows[:, h * DV : (h + 1) * DV],
            preferred_element_type=jnp.float32,
        )
        outs.append((weighted / weight_sum).astype(jnp.bfloat16))
    own_heads = jnp.concatenate(outs, axis=1)
    total = residual.astype(jnp.float32)
    for d, block in enumerate(others(own_heads, "tp")):
        part = take(out_proj, lax.rem(tp_index - d + tp_count, tp_count), tp_count, 0)
        total = total + jnp.dot(block, part, preferred_element_type=jnp.float32)
    mixed_rows = total.astype(jnp.bfloat16)

    result = mixed_rows.astype(jnp.float32)
    for d, rows in enumerate(others(mixed_rows, "z")):
        normed_rows = norm_round(in_order(others(rows, "tp"), "tp", 1), mixer_gain)
        hidden = (
            jax.nn.silu(jnp.dot(normed_rows, gate, preferred_element_type=jnp.float32))
            * jnp.dot(normed_rows, up, preferred_element_type=jnp.float32)
        ).astype(jnp.bfloat16)

        def share(index):
            part = take(down, lax.rem(index, tp_count), tp_count, 0)
            return lax.dot_general(
                hidden, part, (((1,), (1,)), ((), ())), preferred_element_type=jnp.float32
            )

        arrived = [
            hop(share(tp_index + e).astype(jnp.bfloat16), "tp", e) for e in range(1, tp_count)
        ]
        sums = share(tp_index)
        for part in arrived:
            sums = sums + part.astype(jnp.float32)
        if d:
            sums = hop(sums.astype(jnp.bfloat16), "z", -d).astype(jnp.float32)
        result = result + sums
    return result.astype(jnp.bfloat16)


Y, C, X = 2, 2, 2
LANES = 128
MESH = pl.DeviceIdType.MESH
VMEM = pltpu.VMEM
F32, BF16 = jnp.float32, jnp.bfloat16


def nearest(z_count):
    return [
        sorted(range(z_count), key=lambda s: (abs(s - z), s if 2 * z < z_count else -s))
        for z in range(z_count)
    ]


def pick(index, values):
    result = jnp.int32(values[0])
    for k in range(1, len(values)):
        result = jnp.where(index == k, jnp.int32(values[k]), result)
    return result


def split_blocks(blocks, z_count):
    least, left = divmod(blocks, z_count)
    low, high = left - left // 2, left // 2
    return least, low, z_count - high


def rotary_tables(positions):
    inverse = np.float32(10000.0) ** (-np.arange(0, DR, 2, dtype=np.float32) / np.float32(DR))
    angles = positions.astype(np.float32)[:, None] * inverse.astype(np.float32)[None, :]
    wide = angles.astype(np.float64)
    repeat = LANES // (DR // 2)
    return (
        np.tile(np.cos(wide).astype(np.float32), (1, repeat)),
        np.tile(np.sin(wide).astype(np.float32), (1, repeat)),
    )


def turn_matrices():
    middle = DR // 2
    turn = np.zeros((DR, DR), np.float32)
    for i in range(middle):
        turn[middle + i, i] = -1.0
        turn[i, middle + i] = 1.0
    copies = LANES // DR
    same = np.concatenate([np.eye(DR, dtype=np.float32)] * copies, axis=1)
    paired = np.kron(np.eye(copies, dtype=np.float32), turn)
    return same, paired


def layer_kernel(
    z_count,
    qc_ref,
    qr_ref,
    lat_ref,
    krt_ref,
    lgain_ref,
    key_up_ref,
    value_up_ref,
    mgain_ref,
    same_ref,
    paired_ref,
    oproj_hbm,
    res_hbm,
    gate_hbm,
    up_hbm,
    down_hbm,
    cos_hbm,
    sin_hbm,
    out_ref,
    lat_own,
    lat_buf,
    cos_buf,
    sin_buf,
    oproj_buf,
    res_buf,
    gate_buf,
    up_buf,
    down_buf,
    key_s,
    value_s,
    turn_s,
    q_s,
    max_s,
    sum_s,
    acc_s,
    ho_buf,
    mix_s,
    tok_buf,
    nrm_s,
    hid_s,
    part_s,
    fin_s,
    zs_send,
    zs_recv,
    pair_recv,
    xo_send,
    xo_recv,
    loc_sem,
    lz_s,
    lz_r,
    ly_s,
    ly_r,
    lx_s,
    lx_r,
    lc_s,
    lc_r,
    wz_s,
    wz_r,
    wy_s,
    wy_r,
    wx_s,
    wx_r,
    wc_s,
    wc_r,
    x_sem,
    tu_s,
    td_s,
    tz_r,
    rs_s,
    ra_r,
    rb_r,
    rc_r,
    xo_r,
):
    sp, x = lax.axis_index("sp"), lax.axis_index("tp")
    z, y, c = sp // (Y * C), (sp // C) % Y, sp % C
    order = nearest(z_count)
    rows = qc_ref.shape[0]
    per_device = lat_ref.shape[0]
    rank = lat_ref.shape[1]
    chunk = Y * C * X * per_device
    heads = key_up_ref.shape[1] // DN
    depth = gate_hbm.shape[0]
    blocks = gate_hbm.shape[1] // LANES
    least, low, high = split_blocks(blocks, z_count)
    main = least * LANES
    half = res_hbm.shape[1]
    pad = gate_buf.shape[1] // X
    share = rows // X
    cut = C * Y * LANES

    def dev(zz, yy, cc, xx):
        return ((zz * Y + yy) * C + cc, xx)

    def has_extra(zz):
        return (zz < low) | (zz >= high)

    def offset(zz):
        return (zz * least + jnp.minimum(zz, low) + jnp.maximum(zz - high, 0)) * LANES

    def remote(src, dst, send, recv, to):
        return pltpu.make_async_remote_copy(
            src_ref=src,
            dst_ref=dst,
            send_sem=send,
            recv_sem=recv,
            device_id=to,
            device_id_type=MESH,
        )

    y_peer, x_peer, c_peer = dev(z, 1 - y, c, x), dev(z, y, c, 1 - x), dev(z, y, 1 - c, x)

    def each_part(zz, action):
        @pl.when(has_extra(zz))
        def _():
            action(True)

        @pl.when(jnp.logical_not(has_extra(zz)))
        def _():
            action(False)

    slot = sp
    own = offset(z)

    def weight_block(m, index, xx, extra):
        start = pl.multiple_of(xx * pad, LANES)
        span = pl.ds(start, main + LANES if extra else main)
        if m < 2:
            buf = (gate_buf, up_buf)[m]
            return buf.at[pl.ds(pl.multiple_of(index * depth, depth), depth), span]
        return down_buf.at[index, span]

    def weight_source(m, zz, extra):
        start = pl.multiple_of(offset(zz), LANES)
        size = main + LANES if extra else main
        if m < 2:
            return (gate_hbm, up_hbm)[m].at[:, pl.ds(start, size)]
        return down_hbm.at[pl.ds(start, size)]

    locals_ = [
        (lat_own, lat_buf.at[z, c, y, x], 0),
        (cos_hbm, cos_buf, 1),
        (sin_hbm, sin_buf, 2),
        (oproj_hbm, oproj_buf, 3),
        (res_hbm, res_buf, 4),
    ]

    def local(k):
        src, dst, sem = locals_[k]
        return pltpu.make_async_copy(src, dst, loc_sem.at[sem])

    def own_weight(m, extra):
        return pltpu.make_async_copy(
            weight_source(m, z, extra),
            weight_block(m, slot, x, extra),
            loc_sem.at[5 + m],
        )

    lat_own[:, :rank] = lat_ref[...]
    lat_own[:, rank:] = lax.dot_general(
        krt_ref[...], same_ref[...], (((0,), (0,)), ((), ())), preferred_element_type=F32
    ).astype(BF16)
    for k in range(1, len(locals_)):
        local(k).start()
    for m in range(3):
        each_part(z, lambda e: own_weight(m, e).start())

    @pl.when(jnp.logical_not(has_extra(z)))
    def _():
        for xx in range(X):
            tail = slice(xx * pad + main, (xx + 1) * pad)
            gate_buf[:, tail] = jnp.zeros((gate_buf.shape[0], pad - main), BF16)
            up_buf[:, tail] = jnp.zeros((up_buf.shape[0], pad - main), BF16)
            down_buf[:, tail, :] = jnp.zeros((down_buf.shape[0], pad - main, LANES), BF16)

    barrier = pltpu.get_barrier_semaphore()
    for peer in (y_peer, x_peer, c_peer):
        pl.semaphore_signal(barrier, inc=1, device_id=peer, device_id_type=MESH)
    for d in range(1, z_count):
        pl.semaphore_signal(
            barrier,
            inc=1,
            device_id=dev(lax.rem(z + d, z_count), y, c, x),
            device_id_type=MESH,
        )
    with jax.named_scope('entry'):
        pl.semaphore_wait(barrier, 3 + z_count - 1)

    def lat_z(source, target):
        return remote(
            lat_own,
            lat_buf.at[source, c, y, x],
            lz_s.at[target],
            lz_r.at[source],
            dev(target, y, c, x),
        )

    def lat_y(zz, yy):
        block = lat_buf.at[zz, c, yy, x]
        return remote(block, block, ly_s.at[zz], ly_r.at[zz], y_peer)

    def lat_x(zz, xx):
        block = lat_buf.at[zz, c, :, xx]
        return remote(block, block, lx_s.at[zz], lx_r.at[zz], x_peer)

    def lat_c(zz, cc):
        block = lat_buf.at[zz, cc]
        return remote(block, block, lc_s.at[zz], lc_r.at[zz], c_peer)

    local(0).start()
    local(0).wait()
    lat_y(z, y).start()
    for d in range(1, z_count):

        @pl.when(z + d < z_count)
        def _():
            lat_z(z, z + d).start()

    def weight_z(m, source, target, extra, index):
        return remote(
            weight_source(m, target, extra),
            weight_block(m, index, x, extra),
            wz_s.at[target, m],
            wz_r.at[source, m],
            dev(target, y, c, x),
        )

    def at(s):
        return pick(z, [o[s] for o in order])

    def send_z(m, s):
        each_part(at(s), lambda e: weight_z(m, z, at(s), e, slot).start())

    for m in range(2):
        for s in range(1, z_count):
            send_z(m, s)

    def block_of(zz, yy, cc):
        return (zz * Y + yy) * C + cc

    def weight_y(m, zz, yy, xx, hop, extra):
        block = weight_block(m, block_of(zz, yy, c), xx, extra)
        return remote(block, block, wy_s.at[m], wy_r.at[zz, hop, m], y_peer)

    def weight_x(m, zz, yy, xx, hop, extra):
        block = weight_block(m, block_of(zz, yy, c), xx, extra)
        return remote(block, block, wx_s.at[m], wx_r.at[zz, hop, m], x_peer)

    def weight_c(m, zz, yy, xx, cc, extra):
        block = weight_block(m, block_of(zz, yy, cc), xx, extra)
        arrival = wc_r.at[m] if m < 2 else wc_r.at[2 + zz]
        return remote(block, block, wc_s.at[m], arrival, c_peer)

    def y_first(m, s):
        return (False, s % 2 == 1, s % 2 == 0)[m]

    def to_core(m, zz, yy, xx):
        each_part(z, lambda e: weight_c(m, zz, yy, xx, c, e).start())

    def relay_own(m, s):
        zz = at(s)
        if s:
            each_part(z, lambda e: weight_z(m, zz, z, e, block_of(zz, y, c)).wait_recv())
        else:
            each_part(z, lambda e: own_weight(m, e).wait())
        each_part(z, lambda e: weight_y(m, zz, y, x, 0, e).start())
        to_core(m, zz, y, x)

    def relay_own_x(m, s):
        each_part(z, lambda e: weight_x(m, at(s), y, x, 0, e).start())

    def relay_second(m, s):
        zz = at(s)
        if y_first(m, s):
            each_part(z, lambda e: weight_y(m, zz, 1 - y, x, 0, e).wait_recv())
            each_part(z, lambda e: weight_x(m, zz, 1 - y, x, 1, e).start())
            to_core(m, zz, 1 - y, x)
        else:
            each_part(z, lambda e: weight_x(m, zz, y, 1 - x, 0, e).wait_recv())
            each_part(z, lambda e: weight_y(m, zz, y, 1 - x, 1, e).start())
            to_core(m, zz, y, 1 - x)

    def relay_last(m, s):
        zz = at(s)
        if y_first(m, s):
            each_part(z, lambda e: weight_x(m, zz, y, 1 - x, 0, e).wait_recv())
            to_core(m, zz, y, 1 - x)
            each_part(z, lambda e: weight_x(m, zz, 1 - y, 1 - x, 1, e).wait_recv())
        else:
            each_part(z, lambda e: weight_y(m, zz, 1 - y, x, 0, e).wait_recv())
            to_core(m, zz, 1 - y, x)
            each_part(z, lambda e: weight_y(m, zz, 1 - y, 1 - x, 1, e).wait_recv())
        to_core(m, zz, 1 - y, 1 - x)

    pieces = [(0, 0), (1, 0)]
    pieces += [(0, s) for s in range(1, z_count)] + [(1, s) for s in range(1, z_count)]
    pieces += [(2, s) for s in range(z_count)]

    def relay(name, *steps):
        for kind, *ks in steps:
            for k in ks:
                with jax.named_scope(f"{name}_{kind}{k}"):
                    if kind in "ap":
                        relay_own(*pieces[k])
                    if kind in "aq":
                        relay_own_x(*pieces[k])
                    if kind == "b":
                        relay_second(*pieces[k])
                    if kind == "c":
                        relay_last(*pieces[k])

    relay('r0', ('a', 0))
    with jax.named_scope("lat_y_own"):
        lat_y(z, 1 - y).wait_recv()
        lat_x(z, x).start()

    def lower(action):
        for d in range(1, z_count):

            @pl.when(z >= d)
            def _():
                action(z - d)

    def y_step(zz):
        lat_z(zz, z).wait_recv()
        lat_y(zz, y).start()

    def x_step(zz):
        lat_y(zz, 1 - y).wait_recv()
        lat_x(zz, x).start()

    def c_step(zz):
        lat_x(zz, 1 - x).wait_recv()
        lat_c(zz, c).start()

    with jax.named_scope("lat_z"):
        lower(y_step)
    relay('r0', ('p', 1))
    with jax.named_scope("lat_x_own"):
        lat_x(z, 1 - x).wait_recv()
        lat_c(z, c).start()
    with jax.named_scope("lat_y"):
        lower(x_step)

    local(1).wait()
    local(2).wait()
    q_start = pl.multiple_of((c * Y + y) * rows, rows)
    cos_q = cos_buf[z, pl.ds(q_start, rows), :]
    sin_q = sin_buf[z, pl.ds(q_start, rows), :]
    lane = lax.broadcasted_iota(jnp.int32, (rows, LANES), 1)
    for pair in range(heads * DR // LANES):
        start = pl.multiple_of(x * heads * DR + pair * LANES, LANES)
        part = qr_ref[:, pl.ds(start, LANES)]
        swapped = jnp.dot(part, paired_ref[...], preferred_element_type=F32)
        turned = (part.astype(F32) * cos_q + swapped * sin_q).astype(BF16)
        for k in range(LANES // DR):
            h = pair * (LANES // DR) + k
            keep = (lane >= k * DR) & (lane < (k + 1) * DR)
            q_s[h, :, LANES:] = jnp.where(keep, turned, jnp.zeros_like(turned))
    for h in range(heads):
        start = pl.multiple_of(x * heads * DN + h * DN, DN)
        q_s[h, :, :LANES] = qc_ref[:, pl.ds(start, DN)]

    scale = 1.0 / math.sqrt(DN + DR)
    max_s[...] = jnp.full(max_s.shape, masked_score, F32)
    sum_s[...] = jnp.zeros(sum_s.shape, F32)
    acc_s[...] = jnp.zeros(acc_s.shape, F32)
    key_id = lax.broadcasted_iota(jnp.int32, (rows, chunk), 1)
    per_c, per_y = Y * X * per_device, X * per_device
    c_id = key_id // per_c
    y_id = (key_id // per_y) % Y
    key_place = y_id * C * per_y + c_id * per_y + key_id % per_y
    query_place = (y * C + c) * per_y + lax.broadcasted_iota(jnp.int32, (rows, chunk), 0)

    def attend(d):
        zz = z - d
        lat_c(zz, 1 - c).wait_recv()
        both = lat_buf[zz].reshape(chunk, rank + LANES)
        wide = both[:, :rank].astype(F32)
        factor = lax.rsqrt(jnp.mean(wide * wide, axis=-1, keepdims=True) + epsilon)
        normed = (wide * factor * lgain_ref[...]).astype(BF16)
        key_s[...] = jnp.dot(normed, key_up_ref[...], preferred_element_type=F32).astype(BF16)
        value_s[...] = jnp.dot(normed, value_up_ref[...], preferred_element_type=F32).astype(BF16)
        rot = both[:, rank:]
        swapped = jnp.dot(rot, paired_ref[...], preferred_element_type=F32)
        turn_s[...] = (rot.astype(F32) * cos_buf[zz] + swapped * sin_buf[zz]).astype(BF16)
        allowed = (key_place - d * chunk) // SPAN <= query_place // SPAN
        for h in range(heads):
            k = jnp.concatenate([key_s[:, h * DN : (h + 1) * DN], turn_s[...]], axis=1)
            scores = lax.dot_general(
                q_s[h], k, (((1,), (1,)), ((), ())), preferred_element_type=F32
            )
            scores = jnp.where(allowed, scores * scale, masked_score)
            before = max_s[h, :, :1]
            peak = jnp.maximum(before, jnp.max(scores, axis=-1, keepdims=True))
            weights = jnp.exp(scores - peak)
            fade = jnp.exp(before - peak)
            total = sum_s[h, :, :1] * fade + jnp.sum(weights, axis=-1, keepdims=True)
            gained = jnp.dot(
                weights.astype(BF16),
                value_s[:, h * DV : (h + 1) * DV],
                preferred_element_type=F32,
            )
            acc_s[h] = acc_s[h] * fade + gained
            max_s[h] = jnp.broadcast_to(peak, max_s.shape[1:])
            sum_s[h] = jnp.broadcast_to(total, sum_s.shape[1:])

    relay("r1", ("b", 0), ("q", 1), ("a", 8))
    with jax.named_scope("attend0"):
        attend(0)
    with jax.named_scope("lat_x"):
        lower(c_step)
    relay("r2", ("a", 2))
    for d in range(1, z_count):

        @pl.when(z >= d)
        def _():
            with jax.named_scope(f"attend{d}"):
                attend(d)

        if d < z_count - 1:
            if d == 2:
                relay("r3", ("b", 1))

    for h in range(heads):
        ho_buf[x, :, h * DV : (h + 1) * DV] = (acc_s[h] / sum_s[h]).astype(BF16)

    def heads_out(xx):
        return remote(ho_buf.at[xx], ho_buf.at[xx], x_sem.at[0], x_sem.at[1], x_peer)

    heads_out(x).start()
    relay("r5", ("a", 3), ("b", 2), ("p", 4))

    local(3).wait()
    local(4).wait()
    width = heads * DV
    with jax.named_scope("heads_wait"):
        heads_out(1 - x).wait_recv()
    total = res_buf[...].astype(F32)
    for k in range(X):
        total = total + jnp.dot(
            ho_buf[k], oproj_buf[k * width : (k + 1) * width, :], preferred_element_type=F32
        )
    mix_s[...] = total.astype(BF16).reshape(X, share, half)

    def features(xx):
        return pl.ds(pl.multiple_of(xx * half, LANES), half)

    def tok_x(to):
        return remote(
            mix_s.at[to],
            tok_buf.at[z, :, features(1 - to)],
            x_sem.at[2],
            x_sem.at[3],
            x_peer,
        )

    tok_x(1 - x).start()
    tok_buf[z, :, features(x)] = mix_s[x]
    for s in range(1, z_count):
        send_z(2, s)
    relay("r6", ("q", 4), ("b", 3), ("a", 5), ("c", 0, 1))
    with jax.named_scope("tok_x"):
        tok_x(x).wait_recv()

    def tok_z(zz, to, sem):
        block = tok_buf.at[zz]
        return remote(block, block, sem.at[zz], tz_r.at[zz], dev(to, y, c, x))

    def goes_up(zz):
        return (zz <= z) & (z + 1 < z_count)

    def goes_down(zz):
        return (zz >= z) & (z > 0)

    def forward(zz):
        @pl.when(goes_up(zz))
        def _():
            tok_z(zz, z + 1, tu_s).start()

        @pl.when(goes_down(zz))
        def _():
            tok_z(zz, z - 1, td_s).start()

    def relay_tokens(s):
        with jax.named_scope(f"rt{s}"):
            tok_z(at(s), z, tu_s).wait_recv()
            forward(at(s))

    def normalize(s):
        zz = at(s)
        wide = tok_buf[zz].astype(F32)
        factor = lax.rsqrt(jnp.mean(wide * wide, axis=-1, keepdims=True) + epsilon)
        lines = pl.ds(pl.multiple_of(zz * share, share), share)
        nrm_s[lines, :] = (wide * factor * mgain_ref[...]).astype(BF16)

    forward(z)
    relay("r7", ("a", 6), ("b", 4), ("a", 7), ("b", 5), ("c", 2))
    normalize(0)
    relay_tokens(1)
    relay("r8", ("a", 9), ("b", 6, 7), ("c", 3))
    normalize(1)
    relay_tokens(2)
    relay("r9", ("a", 10, 11), ("b", 8), ("c", 4, 5))
    normalize(2)
    relay_tokens(3)
    relay("r10", ("c", 6, 7), ("b", 9))
    normalize(3)

    def wait_core(m):
        ref = (gate_buf, up_buf)[m]

        def wait(e):
            whole = ref.at[:, pl.ds(0, main + LANES if e else main)]
            remote(whole, whole, wc_s.at[m], wc_r.at[m], c_peer).wait_recv()

        each_part(z, wait)

    def wait_down(zz):
        def wait(e):
            whole = down_buf.at[pl.ds(0, X * Y), pl.ds(0, main + LANES if e else main)]
            remote(whole, whole, wc_s.at[2], wc_r.at[2 + zz], c_peer).wait_recv()

        each_part(z, wait)

    with jax.named_scope("wait_gu"):
        for m in range(2):
            wait_core(m)

    wide_tile = 2 * LANES

    def hidden(n, carry):
        lanes = pl.ds(pl.multiple_of(n * wide_tile, wide_tile), wide_tile)
        g = jnp.dot(nrm_s[...], gate_buf[:, lanes], preferred_element_type=F32)
        u = jnp.dot(nrm_s[...], up_buf[:, lanes], preferred_element_type=F32)
        hid_s[:, lanes] = (g / (1.0 + jnp.exp(-g)) * u).astype(BF16)
        return carry

    tiles = X * pad // wide_tile
    with jax.named_scope("hidden_a"):
        lax.fori_loop(0, tiles // 2, hidden, 0)
    relay('r13', ('b', 10))
    with jax.named_scope("hidden_b"):
        lax.fori_loop(tiles // 2, tiles, hidden, 0)

    def columns(zz):
        return pl.ds(pl.multiple_of(zz * cut, cut), cut)

    partner = z + 1 - 2 * (z % 2)
    outer = (z == 0) | (z == z_count - 1)
    across = [2 * (1 - z // 2) + j for j in range(2)]

    def to_partner(zc):
        return remote(
            zs_send.at[0, :, columns(zc)],
            zs_recv.at[0, :, columns(zc)],
            rs_s.at[0],
            ra_r.at[zc],
            dev(partner, y, c, x),
        )

    def to_pair(j, zc):
        return remote(
            zs_send.at[1 + j, :, columns(zc)],
            pair_recv.at[j, :, columns(zc)],
            rs_s.at[1 + j],
            rb_r.at[j, zc],
            dev(partner, y, c, x),
        )

    def to_across(j, zc):
        return remote(
            zs_send.at[1 + j, :, columns(zc)],
            zs_recv.at[1, :, columns(zc)],
            rs_s.at[1 + j],
            rc_r.at[zc],
            dev(across[j], y, c, x),
        )

    def lines_of(zz):
        return pl.ds(pl.multiple_of(zz * share, share), share)

    def chunk_at(i):
        return jnp.where(z < 2, jnp.int32((1, 0, 2, 3)[i]), jnp.int32((2, 3, 1, 0)[i]))

    def mix(i):
        zc = chunk_at(i)
        for n in range(cut // wide_tile):
            first = zc * (Y * C) + 2 * n
            w = jnp.concatenate([down_buf[first], down_buf[first + 1]], axis=1)
            lanes = pl.ds(n * wide_tile, wide_tile)
            part_s[i % 2, :, lanes] = jnp.dot(hid_s[...], w, preferred_element_type=F32)
        @pl.when(outer)
        def _():
            for j in range(2):
                mine = part_s[i % 2, lines_of(across[j]), :]
                zs_send[1 + j, :, columns(zc)] = mine.astype(BF16)
                to_pair(j, zc).start()

        zs_send[0, :, columns(zc)] = part_s[i % 2, lines_of(partner), :].astype(BF16)
        to_partner(zc).start()
        fin_s[:, columns(zc)] = part_s[i % 2, lines_of(z), :] + tok_buf[z, :, columns(zc)].astype(F32)

    def combine(i):
        zc = chunk_at(i)

        @pl.when(jnp.logical_not(outer))
        def _():
            for j in range(2):
                to_pair(j, zc).wait_recv()
                both = part_s[i % 2, lines_of(across[j]), :] + pair_recv[j, :, columns(zc)].astype(F32)
                zs_send[1 + j, :, columns(zc)] = both.astype(BF16)
                to_across(j, zc).start()

    def to_x(zc):
        lanes = pl.ds(pl.multiple_of(zc % 2 * cut, cut), cut)
        return remote(
            xo_send.at[:, lanes], xo_recv.at[:, lanes], x_sem.at[4], xo_r.at[zc % 2], x_peer
        )

    def finish(i):
        zc = chunk_at(i)
        lanes = pl.ds(pl.multiple_of(zc % 2 * cut, cut), cut)
        to_partner(zc).wait_recv()
        to_across(0, zc).wait_recv()
        result = fin_s[:, columns(zc)]
        for k in range(2):
            result = result + zs_recv[k, :, columns(zc)].astype(F32)

        @pl.when(zc // 2 == x)
        def _():
            out_ref[lines_of(x), lanes] = result.astype(BF16)

        @pl.when(zc // 2 != x)
        def _():
            xo_send[:, lanes] = result.astype(BF16)
            to_x(zc).start()

    relay('r14', ('b', 11), ('c', 8, 9))
    def sent(m, send, count):
        def wait(e):
            size = main + LANES if e else main
            if m < 2:
                ref = (gate_buf, up_buf)[m].at[pl.ds(0, count * depth), pl.ds(0, size)]
            else:
                ref = down_buf.at[pl.ds(0, count), pl.ds(0, size)]
            remote(ref, ref, send.at[m], wz_r.at[0, 0], x_peer).wait_send()

        each_part(z, wait)

    def drain():
        tok_x(1 - x).wait_send()
        heads_out(x).wait_send()
        lat_y(z, y).wait_send()
        lat_x(z, x).wait_send()
        lat_c(z, c).wait_send()
        for d in range(1, z_count):

            @pl.when(z + d < z_count)
            def _():
                lat_z(z, z + d).wait_send()

        def lat_done(zz):
            lat_y(zz, y).wait_send()
            lat_x(zz, x).wait_send()
            lat_c(zz, c).wait_send()

        lower(lat_done)
        for m in range(3):
            second_x = sum(y_first(m, s) for s in range(z_count))
            sent(m, wx_s, z_count + second_x)
            sent(m, wy_s, 2 * z_count - second_x)
            sent(m, wc_s, z_count * Y * X)
            for s in range(1, z_count):
                each_part(at(s), lambda e: weight_z(m, z, at(s), e, slot).wait_send())
        for s in range(z_count):
            zz = at(s)

            @pl.when(goes_up(zz))
            def _():
                tok_z(zz, z + 1, tu_s).wait_send()

            @pl.when(goes_down(zz))
            def _():
                tok_z(zz, z - 1, td_s).wait_send()

    for i in range(z_count):
        if i == 1:
            relay("r15", ("c", 10, 11))
        if i in (0, 2):
            with jax.named_scope(f"wait_d{i}"):
                for s in range(i, i + 2):
                    wait_down(at(s))
        with jax.named_scope(f"mix{i}"):
            mix(i)
        if i:
            with jax.named_scope(f"combine{i-1}"):
                combine(i - 1)
    with jax.named_scope("combine_last"):
        combine(z_count - 1)
    with jax.named_scope("drain"):
        drain()
    for i in range(z_count):
        with jax.named_scope(f"finish{i}"):
            finish(i)
    with jax.named_scope("result_x"):
        for k in range(2):
            to_x(jnp.int32(k)).wait_recv()
    out_ref[lines_of(1 - x), :] = xo_recv[...]

    for k in range(3):
        whole = zs_send.at[k]
        remote(whole, whole, rs_s.at[k], xo_r.at[0], x_peer).wait_send()
    remote(xo_send, xo_recv, x_sem.at[4], xo_r.at[0], x_peer).wait_send()


def fits(mesh):
    return mesh.shape["tp"] == X and mesh.shape["sp"] == 4 * Y * C


def fused(mesh):
    sp_count = mesh.shape["sp"]
    z_count = sp_count // (Y * C)

    def shard(
        query_content,
        query_rotary,
        latents,
        key_rotary,
        latent_gain,
        key_up,
        value_up,
        out_proj,
        residual,
        mixer_gain,
        gate_proj,
        up_proj,
        down_proj,
    ):
        rows = query_content.shape[0]
        per_device, rank = latents.shape
        chunk = Y * C * X * per_device
        heads = key_up.shape[1] // DN
        half = residual.shape[1]
        depth, units = gate_proj.shape
        least, low, high = split_blocks(units // LANES, z_count)
        pad = (least + 2 - least % 2) * LANES
        model = X * half
        share = rows // X
        places = np.arange(z_count * chunk).reshape(z_count, Y, C, rows)
        places = places.transpose(0, 2, 1, 3).reshape(-1)
        cosines, sines = (t.reshape(z_count, chunk, LANES) for t in rotary_tables(places))
        same, paired = (jnp.asarray(t, BF16) for t in turn_matrices())
        vmem = pl.BlockSpec(memory_space=VMEM)
        hbm = pl.BlockSpec(memory_space=pl.ANY)
        dma = pltpu.SemaphoreType.DMA
        scratch = [
            VMEM((per_device, rank + LANES), BF16),
            VMEM((z_count, C, Y, X, per_device, rank + LANES), BF16),
            VMEM((z_count, chunk, LANES), F32),
            VMEM((z_count, chunk, LANES), F32),
            VMEM(out_proj.shape, BF16),
            VMEM((rows, half), BF16),
            VMEM((model, X * pad), BF16),
            VMEM((model, X * pad), BF16),
            VMEM((sp_count, X * pad, LANES), BF16),
            VMEM((chunk, heads * DN), BF16),
            VMEM((chunk, heads * DV), BF16),
            VMEM((chunk, LANES), BF16),
            VMEM((heads, rows, 2 * LANES), BF16),
            VMEM((heads, rows, LANES), F32),
            VMEM((heads, rows, LANES), F32),
            VMEM((heads, rows, DV), F32),
            VMEM((X, rows, heads * DV), BF16),
            VMEM((X, share, half), BF16),
            VMEM((z_count, share, model), BF16),
            VMEM((z_count * share, model), BF16),
            VMEM((z_count * share, X * pad), BF16),
            VMEM((2, z_count * share, Y * C * LANES), F32),
            VMEM((share, model), F32),
            VMEM((3, share, model), BF16),
            VMEM((2, share, model), BF16),
            VMEM((2, share, model), BF16),
            VMEM((share, half), BF16),
            VMEM((share, half), BF16),
            dma((8,)),
            *[dma((z_count,)) for _ in range(8)],
            *[dma((z_count, 3)) for _ in range(2)],
            dma((3,)),
            dma((z_count, 2, 3)),
            dma((3,)),
            dma((z_count, 2, 3)),
            dma((3,)),
            dma((2 + z_count,)),
            dma((5,)),
            *[dma((z_count,)) for _ in range(3)],
            dma((3,)),
            dma((z_count,)),
            dma((2, z_count)),
            dma((z_count,)),
            dma((2,)),
        ]
        return pl.pallas_call(
            functools.partial(layer_kernel, z_count),
            out_shape=jax.ShapeDtypeStruct(residual.shape, residual.dtype),
            in_specs=[vmem] * 10 + [hbm] * 7,
            out_specs=vmem,
            scratch_shapes=scratch,
            compiler_params=pltpu.CompilerParams(
                collective_id=0, has_side_effects=True, vmem_limit_bytes=60 * 1024 * 1024
            ),
        )(
            query_content,
            query_rotary,
            latents,
            key_rotary.T,
            latent_gain[None, :],
            key_up,
            value_up,
            mixer_gain[None, :],
            same,
            paired,
            out_proj,
            residual,
            gate_proj,
            up_proj,
            down_proj,
            cosines,
            sines,
        )

    return jax.shard_map(
        shard,
        mesh=mesh,
        in_specs=(
            P("sp", None),
            P("sp", None),
            P(("sp", "tp"), None),
            P(("sp", "tp"), None),
            P(),
            P(None, "tp"),
            P(None, "tp"),
            P(None, "tp"),
            P("sp", "tp"),
            P(),
            P("sp", "tp"),
            P("sp", "tp"),
            P("tp", "sp"),
        ),
        out_specs=P("sp", "tp"),
        check_vma=False,
    )


def plain(mesh):
    sp_count, tp_count = mesh.shape["sp"], mesh.shape["tp"]
    grouped = Mesh(mesh.devices.reshape(sp_count // 4, 2, 2, tp_count), SP + ("tp",))
    return jax.shard_map(
        shards,
        mesh=grouped,
        in_specs=(
            P(SP, None),
            P(SP, None),
            P(SP + ("tp",), None),
            P(SP + ("tp",), None),
            P(),
            P(None, "tp"),
            P(None, "tp"),
            P(None, "tp"),
            P(SP, "tp"),
            P(),
            P(SP, "tp"),
            P(SP, "tp"),
            P("tp", SP),
        ),
        out_specs=P(SP, "tp"),
        check_vma=False,
    )


def solution(mesh):
    if fits(mesh):
        return fused(mesh)
    return plain(mesh)
```

```python
import functools
import math

import jax
import jax.numpy as jnp
import numpy as np
from jax import lax
from jax.experimental import pallas as pl
from jax.experimental.pallas import tpu as pltpu
from jax.sharding import Mesh, PartitionSpec as P

H = 8
DN = 128
DR = 64
DV = 128
SPAN = 64


epsilon = 1e-06
masked_score = -1e30
SP = ("z", "y", "c")


def norm_round(inputs, scales):
    widened = inputs.astype(jnp.float32)
    factor = lax.rsqrt(jnp.mean(widened * widened, axis=-1, keepdims=True) + epsilon)
    return (widened * factor * scales).astype(jnp.bfloat16)


def rotate(inputs, places):
    dimension = inputs.shape[-1]
    middle = dimension // 2
    inverse = 10000.0 ** (-jnp.arange(0, dimension, 2, dtype=jnp.float32) / dimension)
    angles = places.astype(jnp.float32)[:, None, None] * inverse[None, None, :]
    cosine_table = jnp.cos(angles)
    sine_table = jnp.sin(angles)
    widened = inputs.astype(jnp.float32)
    first_half = widened[..., :middle]
    second_half = widened[..., middle:]
    return jnp.concatenate(
        [
            first_half * cosine_table - second_half * sine_table,
            second_half * cosine_table + first_half * sine_table,
        ],
        axis=-1,
    ).astype(jnp.bfloat16)


def hop(inputs, axis, offset):
    count = lax.axis_size(axis)
    return lax.ppermute(inputs, axis, [(i, (i + offset) % count) for i in range(count)])


def others(inputs, axis):
    return [inputs] + [hop(inputs, axis, d) for d in range(1, lax.axis_size(axis))]


def take(inputs, index, count, dim):
    size = inputs.shape[dim] // count
    return lax.dynamic_slice_in_dim(inputs, index * size, size, dim)


def in_order(blocks, axis, dim):
    count, me = lax.axis_size(axis), lax.axis_index(axis)
    if count == 1:
        return blocks[0]
    if count == 2:
        straight = jnp.concatenate(blocks, axis=dim)
        turned = jnp.concatenate(blocks[::-1], axis=dim)
        return jnp.where(me == 0, straight, turned)
    size = blocks[0].shape[dim]
    shape = list(blocks[0].shape)
    shape[dim] = size * count
    result = jnp.zeros(shape, blocks[0].dtype)
    for d, block in enumerate(blocks):
        place = lax.rem(me - d + count, count) * size
        result = lax.dynamic_update_slice_in_dim(result, block, place, dim)
    return result


def shards(
    query_content,
    query_rotary,
    latents,
    key_rotary,
    latent_gain,
    key_up,
    value_up,
    out_proj,
    residual,
    mixer_gain,
    gate_proj,
    up_proj,
    down_proj,
):
    query_rows = query_content.shape[0]
    tp_count, z_count = lax.axis_size("tp"), lax.axis_size("z")
    sp_index, tp_index, z_index = (
        lax.axis_index(SP),
        lax.axis_index("tp"),
        lax.axis_index("z"),
    )
    rank = latents.shape[1]
    per_device = latents.shape[0]
    heads = H // tp_count

    gathered = jnp.concatenate([latents, key_rotary], axis=1)
    places = (sp_index * tp_count + tp_index) * per_device + jnp.arange(
        per_device, dtype=jnp.int32
    )
    strides = {
        "z": lax.axis_size("y") * lax.axis_size("c") * tp_count * per_device,
        "y": lax.axis_size("c") * tp_count * per_device,
        "c": tp_count * per_device,
        "tp": per_device,
    }
    pieces = []
    for weights in (gate_proj, up_proj, down_proj.T):
        rows, columns = weights.shape
        pieces.append(jnp.swapaxes(weights.reshape(rows, z_count, columns // z_count), 0, 1))
    for axis in ("z", "tp", "y", "c"):
        count, me = lax.axis_size(axis), lax.axis_index(axis)
        gathered = jnp.concatenate(others(gathered, axis), axis=0)
        places = jnp.concatenate(
            [places + (lax.rem(me - d + count, count) - me) * strides[axis] for d in range(count)]
        )
        if axis == "z":
            gathered, pieces = lax.optimization_barrier((gathered, pieces))

    whole = []
    for piece in pieces:
        rows, units = piece.shape[1:]
        blocks = []
        for d in range(z_count):
            block = take(piece, lax.rem(z_index + d, z_count), z_count, 0)
            blocks.append(hop(block, "z", d) if d else block)
        block = in_order(blocks, "z", 0)[:, None]
        block = in_order(others(block, "y"), "y", 1)[:, :, None]
        block = in_order(others(block, "c"), "c", 2)
        whole.append(block.reshape(-1, units))
    gate, up, down = whole

    query_places = sp_index * query_rows + jnp.arange(query_rows, dtype=jnp.int32)
    normed = norm_round(gathered[:, :rank], latent_gain)
    key_turned = rotate(gathered[:, None, rank:], places)[:, 0, :]
    own_rotary = take(query_rotary, tp_index, tp_count, 1)
    own_content = take(query_content, tp_index, tp_count, 1)
    query_turned = rotate(own_rotary.reshape(query_rows, heads, DR), query_places)
    allowed = places[None, :] // SPAN <= query_places[:, None] // SPAN
    score_scale = 1.0 / math.sqrt(DN + DR)
    key_rows = jnp.dot(normed, key_up, preferred_element_type=jnp.float32).astype(jnp.bfloat16)
    value_rows = jnp.dot(normed, value_up, preferred_element_type=jnp.float32).astype(jnp.bfloat16)
    outs = []
    for h in range(heads):
        k = jnp.concatenate([key_rows[:, h * DN : (h + 1) * DN], key_turned], axis=1)
        q = jnp.concatenate(
            [own_content[:, h * DN : (h + 1) * DN], query_turned[:, h, :]], axis=1
        )
        scores = lax.dot_general(
            q, k, (((1,), (1,)), ((), ())), preferred_element_type=jnp.float32
        )
        scores = jnp.where(allowed, scores * score_scale, masked_score)
        highest = jnp.max(scores, axis=-1, keepdims=True)
        weights = jnp.where(allowed, jnp.exp(scores - highest), 0.0)
        weight_sum = jnp.sum(weights, axis=-1, keepdims=True)
        weighted = jnp.dot(
            weights.astype(jnp.bfloat16),
            value_rows[:, h * DV : (h + 1) * DV],
            preferred_element_type=jnp.float32,
        )
        outs.append((weighted / weight_sum).astype(jnp.bfloat16))
    own_heads = jnp.concatenate(outs, axis=1)
    total = residual.astype(jnp.float32)
    for d, block in enumerate(others(own_heads, "tp")):
        part = take(out_proj, lax.rem(tp_index - d + tp_count, tp_count), tp_count, 0)
        total = total + jnp.dot(block, part, preferred_element_type=jnp.float32)
    mixed_rows = total.astype(jnp.bfloat16)

    result = mixed_rows.astype(jnp.float32)
    for d, rows in enumerate(others(mixed_rows, "z")):
        normed_rows = norm_round(in_order(others(rows, "tp"), "tp", 1), mixer_gain)
        hidden = (
            jax.nn.silu(jnp.dot(normed_rows, gate, preferred_element_type=jnp.float32))
            * jnp.dot(normed_rows, up, preferred_element_type=jnp.float32)
        ).astype(jnp.bfloat16)

        def share(index):
            part = take(down, lax.rem(index, tp_count), tp_count, 0)
            return lax.dot_general(
                hidden, part, (((1,), (1,)), ((), ())), preferred_element_type=jnp.float32
            )

        arrived = [
            hop(share(tp_index + e).astype(jnp.bfloat16), "tp", e) for e in range(1, tp_count)
        ]
        sums = share(tp_index)
        for part in arrived:
            sums = sums + part.astype(jnp.float32)
        if d:
            sums = hop(sums.astype(jnp.bfloat16), "z", -d).astype(jnp.float32)
        result = result + sums
    return result.astype(jnp.bfloat16)


Y, C, X = 2, 2, 2
LANES = 128
MESH = pl.DeviceIdType.MESH
VMEM = pltpu.VMEM
F32, BF16 = jnp.float32, jnp.bfloat16


def nearest(z_count):
    return [
        sorted(range(z_count), key=lambda s: (abs(s - z), s if 2 * z < z_count else -s))
        for z in range(z_count)
    ]


def pick(index, values):
    result = jnp.int32(values[0])
    for k in range(1, len(values)):
        result = jnp.where(index == k, jnp.int32(values[k]), result)
    return result


def split_blocks(blocks, z_count):
    least, left = divmod(blocks, z_count)
    return least, left - left // 2, z_count - left // 2


def rotary_tables(positions):
    inverse = np.float32(10000.0) ** (-np.arange(0, DR, 2, dtype=np.float32) / np.float32(DR))
    angles = positions.astype(np.float32)[:, None] * inverse.astype(np.float32)[None, :]
    wide = angles.astype(np.float64)
    repeat = LANES // (DR // 2)
    return (
        np.tile(np.cos(wide).astype(np.float32), (1, repeat)),
        np.tile(np.sin(wide).astype(np.float32), (1, repeat)),
    )


def turn_matrices():
    middle = DR // 2
    turn = np.zeros((DR, DR), np.float32)
    for i in range(middle):
        turn[middle + i, i] = -1.0
        turn[i, middle + i] = 1.0
    copies = LANES // DR
    same = np.concatenate([np.eye(DR, dtype=np.float32)] * copies, axis=1)
    paired = np.kron(np.eye(copies, dtype=np.float32), turn)
    return same, paired


def layer_kernel(
    z_count,
    qc_ref,
    qr_ref,
    lat_ref,
    krt_ref,
    lgain_ref,
    key_up_ref,
    value_up_ref,
    mgain_ref,
    same_ref,
    paired_ref,
    oproj_hbm,
    res_hbm,
    gate_hbm,
    up_hbm,
    down_hbm,
    cos_hbm,
    sin_hbm,
    out_ref,
    lat_own,
    lat_buf,
    cos_buf,
    sin_buf,
    oproj_buf,
    res_buf,
    gate_buf,
    up_buf,
    down_buf,
    key_s,
    value_s,
    turn_s,
    q_s,
    max_s,
    sum_s,
    acc_s,
    ho_buf,
    mix_s,
    tok_buf,
    nrm_s,
    hid_s,
    part_s,
    fin_s,
    zs_send,
    zs_recv,
    pair_recv,
    xo_send,
    xo_recv,
    loc_sem,
    lz_s,
    lz_r,
    ly_s,
    ly_r,
    lx_s,
    lx_r,
    lc_s,
    lc_r,
    wz_s,
    wz_r,
    wy_s,
    wy_r,
    wx_s,
    wx_r,
    wc_s,
    wc_r,
    x_sem,
    tu_s,
    td_s,
    tz_r,
    rs_s,
    ra_r,
    rb_r,
    rc_r,
    xo_r,
):
    sp, x = lax.axis_index("sp"), lax.axis_index("tp")
    z, y, c = sp // (Y * C), (sp // C) % Y, sp % C
    order = nearest(z_count)
    rows = qc_ref.shape[0]
    per_device = lat_ref.shape[0]
    rank = lat_ref.shape[1]
    chunk = Y * C * X * per_device
    heads = key_up_ref.shape[1] // DN
    depth = gate_hbm.shape[0]
    blocks = gate_hbm.shape[1] // LANES
    least, low, high = split_blocks(blocks, z_count)
    main = least * LANES
    half = res_hbm.shape[1]
    pad = gate_buf.shape[1] // X
    share = rows // X
    cut = C * Y * LANES

    def dev(zz, yy, cc, xx):
        return ((zz * Y + yy) * C + cc, xx)

    def has_extra(zz, xx):
        ends = (zz < low) | (zz >= high)
        return jnp.where(ends, 1, 0) + xx == 1

    def offset(zz, xx):
        before = jnp.minimum(zz, low) + jnp.maximum(zz - high, 0)
        return (zz * least + before + xx * (zz - 2 * before)) * LANES

    def remote(src, dst, send, recv, to):
        return pltpu.make_async_remote_copy(
            src_ref=src,
            dst_ref=dst,
            send_sem=send,
            recv_sem=recv,
            device_id=to,
            device_id_type=MESH,
        )

    y_peer, x_peer, c_peer = dev(z, 1 - y, c, x), dev(z, y, c, 1 - x), dev(z, y, 1 - c, x)

    def each_part(zz, action, xx=x):
        @pl.when(has_extra(zz, xx))
        def _():
            action(True)

        @pl.when(jnp.logical_not(has_extra(zz, xx)))
        def _():
            action(False)

    slot = sp

    def weight_block(m, index, xx, extra):
        start = pl.multiple_of(xx * pad, LANES)
        span = pl.ds(start, main + LANES if extra else main)
        if m < 2:
            buf = (gate_buf, up_buf)[m]
            return buf.at[pl.ds(pl.multiple_of(index * depth, depth), depth), span]
        return down_buf.at[index, span]

    def weight_source(m, zz, extra):
        start = pl.multiple_of(offset(zz, x), LANES)
        size = main + LANES if extra else main
        if m < 2:
            return (gate_hbm, up_hbm)[m].at[:, pl.ds(start, size)]
        return down_hbm.at[pl.ds(start, size)]

    locals_ = [
        (lat_own, lat_buf.at[z, c, y, x], 0),
        (cos_hbm, cos_buf, 1),
        (sin_hbm, sin_buf, 2),
        (oproj_hbm, oproj_buf, 3),
        (res_hbm, res_buf, 4),
    ]

    def local(k):
        src, dst, sem = locals_[k]
        return pltpu.make_async_copy(src, dst, loc_sem.at[sem])

    def own_weight(m, extra):
        return pltpu.make_async_copy(
            weight_source(m, z, extra),
            weight_block(m, slot, x, extra),
            loc_sem.at[5 + m],
        )

    lat_own[:, :rank] = lat_ref[...]
    lat_own[:, rank:] = lax.dot_general(
        krt_ref[...], same_ref[...], (((0,), (0,)), ((), ())), preferred_element_type=F32
    ).astype(BF16)
    for k in range(1, len(locals_)):
        local(k).start()
    for m in range(3):
        each_part(z, lambda e: own_weight(m, e).start())

    for xx in range(X):

        @pl.when(jnp.logical_not(has_extra(z, xx)))
        def _():
            tail = slice(xx * pad + main, (xx + 1) * pad)
            gate_buf[:, tail] = jnp.zeros((gate_buf.shape[0], pad - main), BF16)
            up_buf[:, tail] = jnp.zeros((up_buf.shape[0], pad - main), BF16)
            down_buf[:, tail, :] = jnp.zeros((down_buf.shape[0], pad - main, LANES), BF16)

    barrier = pltpu.get_barrier_semaphore()
    for peer in (y_peer, x_peer, c_peer):
        pl.semaphore_signal(barrier, inc=1, device_id=peer, device_id_type=MESH)
    for d in range(1, z_count):
        pl.semaphore_signal(
            barrier,
            inc=1,
            device_id=dev(lax.rem(z + d, z_count), y, c, x),
            device_id_type=MESH,
        )
    with jax.named_scope('entry'):
        pl.semaphore_wait(barrier, 3 + z_count - 1)

    def lat_z(source, target):
        return remote(
            lat_own,
            lat_buf.at[source, c, y, x],
            lz_s.at[target],
            lz_r.at[source],
            dev(target, y, c, x),
        )

    def lat_y(zz, yy):
        block = lat_buf.at[zz, c, yy, x]
        return remote(block, block, ly_s.at[zz], ly_r.at[zz], y_peer)

    def lat_x(zz, xx):
        block = lat_buf.at[zz, c, :, xx]
        return remote(block, block, lx_s.at[zz], lx_r.at[zz], x_peer)

    def lat_c(zz, cc):
        block = lat_buf.at[zz, cc]
        return remote(block, block, lc_s.at[zz], lc_r.at[zz], c_peer)

    local(0).start()
    local(0).wait()
    lat_y(z, y).start()
    for d in range(1, z_count):

        @pl.when(z + d < z_count)
        def _():
            lat_z(z, z + d).start()

    def weight_z(m, source, target, extra, index):
        return remote(
            weight_source(m, target, extra),
            weight_block(m, index, x, extra),
            wz_s.at[target, m],
            wz_r.at[source, m],
            dev(target, y, c, x),
        )

    def at(s):
        return pick(z, [o[s] for o in order])

    def send_z(m, s):
        each_part(at(s), lambda e: weight_z(m, z, at(s), e, slot).start())

    for m in range(2):
        for s in range(1, z_count):
            send_z(m, s)

    def block_of(zz, yy, cc):
        return (zz * Y + yy) * C + cc

    def weight_y(m, zz, yy, xx, hop, extra):
        block = weight_block(m, block_of(zz, yy, c), xx, extra)
        return remote(block, block, wy_s.at[hop, m], wy_r.at[zz, hop, m], y_peer)

    def weight_x(m, zz, yy, xx, hop, extra):
        block = weight_block(m, block_of(zz, yy, c), xx, extra)
        return remote(block, block, wx_s.at[hop, m], wx_r.at[zz, hop, m], x_peer)

    def weight_c(m, zz, yy, xx, cc, extra):
        block = weight_block(m, block_of(zz, yy, cc), xx, extra)
        arrival = wc_r.at[m] if m < 2 else wc_r.at[2 + zz]
        return remote(block, block, wc_s.at[m], arrival, c_peer)

    def y_first(m, s):
        return (False, s % 2 == 1, s % 2 == 1)[m]

    def to_core(m, zz, yy, xx):
        each_part(z, lambda e: weight_c(m, zz, yy, xx, c, e).start(), xx)

    def relay_own(m, s):
        zz = at(s)
        if s:
            each_part(z, lambda e: weight_z(m, zz, z, e, block_of(zz, y, c)).wait_recv())
        else:
            each_part(z, lambda e: own_weight(m, e).wait())
        each_part(z, lambda e: weight_y(m, zz, y, x, 0, e).start())
        to_core(m, zz, y, x)

    def relay_own_x(m, s):
        each_part(z, lambda e: weight_x(m, at(s), y, x, 0, e).start())

    def relay_second(m, s):
        zz = at(s)
        if y_first(m, s):
            each_part(z, lambda e: weight_y(m, zz, 1 - y, x, 0, e).wait_recv())
            each_part(z, lambda e: weight_x(m, zz, 1 - y, x, 1, e).start())
            to_core(m, zz, 1 - y, x)
        else:
            each_part(z, lambda e: weight_x(m, zz, y, 1 - x, 0, e).wait_recv(), 1 - x)
            each_part(z, lambda e: weight_y(m, zz, y, 1 - x, 1, e).start(), 1 - x)
            to_core(m, zz, y, 1 - x)

    def relay_last(m, s):
        zz = at(s)
        if y_first(m, s):
            each_part(z, lambda e: weight_x(m, zz, y, 1 - x, 0, e).wait_recv(), 1 - x)
            to_core(m, zz, y, 1 - x)
            each_part(z, lambda e: weight_x(m, zz, 1 - y, 1 - x, 1, e).wait_recv(), 1 - x)
        else:
            each_part(z, lambda e: weight_y(m, zz, 1 - y, x, 0, e).wait_recv())
            to_core(m, zz, 1 - y, x)
            each_part(z, lambda e: weight_y(m, zz, 1 - y, 1 - x, 1, e).wait_recv(), 1 - x)
        to_core(m, zz, 1 - y, 1 - x)

    pieces = [(0, 0), (1, 0)]
    pieces += [(0, s) for s in range(1, z_count)] + [(1, s) for s in range(1, z_count)]
    pieces += [(2, s) for s in range(z_count)]

    def relay(name, *steps):
        for kind, *ks in steps:
            for k in ks:
                with jax.named_scope(f"{name}_{kind}{k}"):
                    if kind in "ap":
                        relay_own(*pieces[k])
                    if kind in "aq":
                        relay_own_x(*pieces[k])
                    if kind == "b":
                        relay_second(*pieces[k])
                    if kind == "c":
                        relay_last(*pieces[k])

    relay('r0', ('a', 0))
    with jax.named_scope("lat_y_own"):
        lat_y(z, 1 - y).wait_recv()
        lat_x(z, x).start()

    def lower(action):
        for d in range(1, z_count):

            @pl.when(z >= d)
            def _():
                action(z - d)

    def y_step(zz):
        lat_z(zz, z).wait_recv()
        lat_y(zz, y).start()

    def x_step(zz):
        lat_y(zz, 1 - y).wait_recv()
        lat_x(zz, x).start()

    def c_step(zz):
        lat_x(zz, 1 - x).wait_recv()
        lat_c(zz, c).start()

    with jax.named_scope("lat_z"):
        lower(y_step)
    relay('r0', ('p', 1))
    with jax.named_scope("lat_x_own"):
        lat_x(z, 1 - x).wait_recv()
        lat_c(z, c).start()

    local(1).wait()
    local(2).wait()
    q_start = pl.multiple_of((c * Y + y) * rows, rows)
    cos_q = cos_buf[z, pl.ds(q_start, rows), :]
    sin_q = sin_buf[z, pl.ds(q_start, rows), :]
    lane = lax.broadcasted_iota(jnp.int32, (rows, LANES), 1)
    for pair in range(heads * DR // LANES):
        start = pl.multiple_of(x * heads * DR + pair * LANES, LANES)
        part = qr_ref[:, pl.ds(start, LANES)]
        swapped = jnp.dot(part, paired_ref[...], preferred_element_type=F32)
        turned = (part.astype(F32) * cos_q + swapped * sin_q).astype(BF16)
        for k in range(LANES // DR):
            h = pair * (LANES // DR) + k
            keep = (lane >= k * DR) & (lane < (k + 1) * DR)
            q_s[h, :, LANES:] = jnp.where(keep, turned, jnp.zeros_like(turned))
    for h in range(heads):
        start = pl.multiple_of(x * heads * DN + h * DN, DN)
        q_s[h, :, :LANES] = qc_ref[:, pl.ds(start, DN)]

    scale = 1.0 / math.sqrt(DN + DR)
    max_s[...] = jnp.full(max_s.shape, masked_score, F32)
    sum_s[...] = jnp.zeros(sum_s.shape, F32)
    acc_s[...] = jnp.zeros(acc_s.shape, F32)
    key_id = lax.broadcasted_iota(jnp.int32, (rows, chunk), 1)
    per_c, per_y = Y * X * per_device, X * per_device
    c_id = key_id // per_c
    y_id = (key_id // per_y) % Y
    key_place = y_id * C * per_y + c_id * per_y + key_id % per_y
    query_place = (y * C + c) * per_y + lax.broadcasted_iota(jnp.int32, (rows, chunk), 0)

    def attend(d):
        zz = z - d
        lat_c(zz, 1 - c).wait_recv()
        both = lat_buf[zz].reshape(chunk, rank + LANES)
        wide = both[:, :rank].astype(F32)
        factor = lax.rsqrt(jnp.mean(wide * wide, axis=-1, keepdims=True) + epsilon)
        normed = (wide * factor * lgain_ref[...]).astype(BF16)
        key_s[...] = jnp.dot(normed, key_up_ref[...], preferred_element_type=F32).astype(BF16)
        value_s[...] = jnp.dot(normed, value_up_ref[...], preferred_element_type=F32).astype(BF16)
        rot = both[:, rank:]
        swapped = jnp.dot(rot, paired_ref[...], preferred_element_type=F32)
        turn_s[...] = (rot.astype(F32) * cos_buf[zz] + swapped * sin_buf[zz]).astype(BF16)
        allowed = (key_place - d * chunk) // SPAN <= query_place // SPAN
        for h in range(heads):
            k = jnp.concatenate([key_s[:, h * DN : (h + 1) * DN], turn_s[...]], axis=1)
            scores = lax.dot_general(
                q_s[h], k, (((1,), (1,)), ((), ())), preferred_element_type=F32
            )
            if d:
                scores = scores * scale
            else:
                scores = jnp.where(allowed, scores * scale, masked_score)
            before = max_s[h, :, :1]
            peak = jnp.maximum(before, jnp.max(scores, axis=-1, keepdims=True))
            weights = jnp.exp(scores - peak)
            fade = jnp.exp(before - peak)
            total = sum_s[h, :, :1] * fade + jnp.sum(weights, axis=-1, keepdims=True)
            gained = jnp.dot(
                weights.astype(BF16),
                value_s[:, h * DV : (h + 1) * DV],
                preferred_element_type=F32,
            )
            acc_s[h] = acc_s[h] * fade + gained
            max_s[h] = jnp.broadcast_to(peak, max_s.shape[1:])
            sum_s[h] = jnp.broadcast_to(total, sum_s.shape[1:])

    with jax.named_scope("lat_y"):
        lower(x_step)
    relay("r1", ("b", 0), ("q", 1), ("p", 8))
    with jax.named_scope("attend0"):
        attend(0)
    with jax.named_scope("lat_x"):
        lower(c_step)
    relay("r2", ("a", 2))
    for d in range(1, z_count):

        @pl.when(z >= d)
        def _():
            with jax.named_scope(f"attend{d}"):
                attend(d)

        if d < z_count - 1:
            if d == 2:
                relay("r3", ("b", 1))

    for h in range(heads):
        ho_buf[x, :, h * DV : (h + 1) * DV] = (acc_s[h] / sum_s[h]).astype(BF16)

    def heads_out(xx):
        return remote(ho_buf.at[xx], ho_buf.at[xx], x_sem.at[0], x_sem.at[1], x_peer)

    heads_out(x).start()
    relay("r5", ("a", 3), ("p", 4))

    local(3).wait()
    local(4).wait()
    width = heads * DV
    with jax.named_scope("heads_wait"):
        heads_out(1 - x).wait_recv()
    total = res_buf[...].astype(F32)
    for k in range(X):
        total = total + jnp.dot(
            ho_buf[k], oproj_buf[k * width : (k + 1) * width, :], preferred_element_type=F32
        )
    mix_s[...] = total.astype(BF16).reshape(X, share, half)

    def features(xx):
        return pl.ds(pl.multiple_of(xx * half, LANES), half)

    def tok_x(to):
        return remote(
            mix_s.at[to],
            tok_buf.at[z, :, features(1 - to)],
            x_sem.at[2],
            x_sem.at[3],
            x_peer,
        )

    tok_x(1 - x).start()
    tok_buf[z, :, features(x)] = mix_s[x]
    outer = (z == 0) | (z == z_count - 1)
    send_z(2, 1)

    @pl.when(outer)
    def _():
        for s in range(2, z_count):
            send_z(2, s)

    relay("r6", ("b", 2), ("q", 4), ("b", 3), ("a", 5), ("c", 0, 1))
    with jax.named_scope("tok_x"):
        tok_x(x).wait_recv()

    def tok_z(zz, to, sem):
        block = tok_buf.at[zz]
        return remote(block, block, sem.at[zz], tz_r.at[zz], dev(to, y, c, x))

    def goes_up(zz):
        return (zz <= z) & (z + 1 < z_count)

    def goes_down(zz):
        return (zz >= z) & (z > 0)

    def forward(zz):
        @pl.when(goes_up(zz))
        def _():
            tok_z(zz, z + 1, tu_s).start()

        @pl.when(goes_down(zz))
        def _():
            tok_z(zz, z - 1, td_s).start()

    def relay_tokens(zz, name):
        with jax.named_scope(f"rt_{name}"):
            tok_z(zz, z, tu_s).wait_recv()
            forward(zz)

    def normalize(s):
        zz = at(s)
        wide = tok_buf[zz].astype(F32)
        factor = lax.rsqrt(jnp.mean(wide * wide, axis=-1, keepdims=True) + epsilon)
        lines = pl.ds(pl.multiple_of(zz * share, share), share)
        nrm_s[lines, :] = (wide * factor * mgain_ref[...]).astype(BF16)

    forward(z)
    relay("r7", ("a", 6), ("b", 4), ("a", 7), ("c", 2))
    normalize(0)
    inner = jnp.logical_not(outer)

    @pl.when(inner)
    def _():
        relay_tokens(z - 1, "below")

    relay("r7", ("b", 5))

    @pl.when(inner)
    def _():
        relay_tokens(z + 1, "above")
        for s in range(2, z_count):
            send_z(2, s)

    relay("r8", ("b", 6), ("q", 8), ("p", 9))

    @pl.when(inner)
    def _():
        relay_tokens(at(3), "far")

    relay("r8", ("b", 7), ("c", 3), ("q", 9))
    @pl.when(inner)
    def _():
        relay("r9", ("c", 4, 5), ("a", 10), ("c", 6), ("a", 11), ("c", 7), ("b", 8))

    @pl.when(outer)
    def _():
        relay("r9", ("c", 4, 5, 6, 7), ("a", 10), ("b", 8), ("a", 11))
        for s in range(1, z_count):
            relay_tokens(at(s), f"{s}")

    for s in range(1, z_count):
        normalize(s)

    both_widths = 2 * main + LANES

    def wait_core(m):
        lines = z_count * Y * X // 2 * depth
        whole = (gate_buf, up_buf)[m].at[pl.ds(0, lines), pl.ds(0, both_widths)]
        remote(whole, whole, wc_s.at[m], wc_r.at[m], c_peer).wait_recv()

    def wait_down(zz):
        whole = down_buf.at[pl.ds(0, X * Y // 2), pl.ds(0, both_widths)]
        remote(whole, whole, wc_s.at[2], wc_r.at[2 + zz], c_peer).wait_recv()

    with jax.named_scope("wait_gu"):
        for m in range(2):
            wait_core(m)

    wide_tile = 2 * LANES

    def hidden(n, carry):
        lanes = pl.ds(pl.multiple_of(n * wide_tile, wide_tile), wide_tile)
        g = jnp.dot(nrm_s[...], gate_buf[:, lanes], preferred_element_type=F32)
        u = jnp.dot(nrm_s[...], up_buf[:, lanes], preferred_element_type=F32)
        hid_s[:, lanes] = (g / (1.0 + jnp.exp(-g)) * u).astype(BF16)
        return carry

    tiles = X * pad // wide_tile
    with jax.named_scope("hidden_a"):
        lax.fori_loop(0, tiles // 2, hidden, 0)
    relay('r13', ('b', 9, 10))
    with jax.named_scope("hidden_b"):
        lax.fori_loop(tiles // 2, tiles, hidden, 0)

    def columns(zz):
        return pl.ds(pl.multiple_of(zz * cut, cut), cut)

    partner = z + 1 - 2 * (z % 2)
    across = [2 * (1 - z // 2) + j for j in range(2)]

    def to_partner(zc):
        return remote(
            zs_send.at[0, :, columns(zc)],
            zs_recv.at[0, :, columns(zc)],
            rs_s.at[0],
            ra_r.at[zc],
            dev(partner, y, c, x),
        )

    def to_pair(j, zc):
        return remote(
            zs_send.at[1 + j, :, columns(zc)],
            pair_recv.at[j, :, columns(zc)],
            rs_s.at[1 + j],
            rb_r.at[j, zc],
            dev(partner, y, c, x),
        )

    def to_across(j, zc):
        return remote(
            zs_send.at[1 + j, :, columns(zc)],
            zs_recv.at[1, :, columns(zc)],
            rs_s.at[1 + j],
            rc_r.at[zc],
            dev(across[j], y, c, x),
        )

    def lines_of(zz):
        return pl.ds(pl.multiple_of(zz * share, share), share)

    early = (((0, 2, 3, 1), (1, 2, 3, 0), (2, 3, 1, 0), (3, 2, 1, 0)),
             ((0, 1, 2, 3), (1, 0, 2, 3), (2, 1, 0, 3), (3, 1, 0, 2)))

    def chunk_at(zz, i):
        return jnp.where(
            x == 0,
            pick(zz, [early[0][k][i] for k in range(z_count)]),
            pick(zz, [early[1][k][i] for k in range(z_count)]),
        )

    def mix(i):
        zc = chunk_at(z, i)
        for n in range(cut // wide_tile):
            first = zc * (Y * C) + 2 * n
            w = jnp.concatenate([down_buf[first], down_buf[first + 1]], axis=1)
            lanes = pl.ds(n * wide_tile, wide_tile)
            part_s[zc, :, lanes] = jnp.dot(hid_s[...], w, preferred_element_type=F32)
        @pl.when(outer)
        def _():
            for j in range(2):
                mine = part_s[zc, lines_of(across[j]), :]
                zs_send[1 + j, :, columns(zc)] = mine.astype(BF16)
                to_pair(j, zc).start()

        zs_send[0, :, columns(zc)] = part_s[zc, lines_of(partner), :].astype(BF16)

        if i == 0:
            to_partner(zc).start()
        else:

            @pl.when(inner)
            def _():
                to_partner(zc).start()

        fin_s[:, columns(zc)] = part_s[zc, lines_of(z), :] + tok_buf[z, :, columns(zc)].astype(F32)

    def combine(i):
        zc = chunk_at(jnp.where(z < 2, 0, z_count - 1), i)

        @pl.when(jnp.logical_not(outer))
        def _():
            for j in range(2):
                to_pair(j, zc).wait_recv()
                both = part_s[zc, lines_of(across[j]), :] + pair_recv[j, :, columns(zc)].astype(F32)
                zs_send[1 + j, :, columns(zc)] = both.astype(BF16)
                to_across(j, zc).start()

    def to_x(zc):
        lanes = pl.ds(pl.multiple_of(zc % 2 * cut, cut), cut)
        return remote(
            xo_send.at[:, lanes], xo_recv.at[:, lanes], x_sem.at[4], xo_r.at[zc % 2], x_peer
        )

    def finish(i):
        zc = chunk_at(jnp.where((z < 2) == outer, z_count - 1, 0), i)
        lanes = pl.ds(pl.multiple_of(zc % 2 * cut, cut), cut)
        to_partner(zc).wait_recv()
        to_across(0, zc).wait_recv()
        result = fin_s[:, columns(zc)]
        for k in range(2):
            result = result + zs_recv[k, :, columns(zc)].astype(F32)

        @pl.when(zc // 2 == x)
        def _():
            out_ref[lines_of(x), lanes] = result.astype(BF16)

        @pl.when(zc // 2 != x)
        def _():
            xo_send[:, lanes] = result.astype(BF16)
            to_x(zc).start()

    def sent(m, sem, count, xx):
        def wait(e):
            size = main + LANES if e else main
            if m < 2:
                ref = (gate_buf, up_buf)[m].at[pl.ds(0, count * depth), pl.ds(0, size)]
            else:
                ref = down_buf.at[pl.ds(0, count), pl.ds(0, size)]
            remote(ref, ref, sem, wz_r.at[0, 0], x_peer).wait_send()

        if count:
            each_part(z, wait, xx)

    def sent_core(m):
        count = z_count * Y * X // 2
        if m < 2:
            ref = (gate_buf, up_buf)[m].at[pl.ds(0, count * depth), pl.ds(0, both_widths)]
        else:
            ref = down_buf.at[pl.ds(0, count), pl.ds(0, both_widths)]
        remote(ref, ref, wc_s.at[m], wz_r.at[0, 0], x_peer).wait_send()

    def drain():
        tok_x(1 - x).wait_send()
        heads_out(x).wait_send()
        lat_y(z, y).wait_send()
        lat_x(z, x).wait_send()
        lat_c(z, c).wait_send()
        for d in range(1, z_count):

            @pl.when(z + d < z_count)
            def _():
                lat_z(z, z + d).wait_send()

        def lat_done(zz):
            lat_y(zz, y).wait_send()
            lat_x(zz, x).wait_send()
            lat_c(zz, c).wait_send()

        lower(lat_done)
        for m in range(3):
            second_x = sum(y_first(m, s) for s in range(z_count))
            sent(m, wx_s.at[0, m], z_count, x)
            sent(m, wx_s.at[1, m], second_x, x)
            sent(m, wy_s.at[0, m], z_count, x)
            sent(m, wy_s.at[1, m], z_count - second_x, 1 - x)
            sent_core(m)
            for s in range(1, z_count):
                each_part(at(s), lambda e: weight_z(m, z, at(s), e, slot).wait_send())
        for s in range(z_count):
            zz = at(s)

            @pl.when(goes_up(zz))
            def _():
                tok_z(zz, z + 1, tu_s).wait_send()

            @pl.when(goes_down(zz))
            def _():
                tok_z(zz, z - 1, td_s).wait_send()

    relay("r13", ("c", 8))
    for i in range(z_count):
        if i == 1:
            relay("r14", ("b", 11), ("c", 9, 10))
        if i == 2:
            relay("r15", ("c", 11))
        with jax.named_scope(f"wait_d{i}"):
            wait_down(chunk_at(z, i))
        with jax.named_scope(f"mix{i}"):
            mix(i)

    @pl.when(outer)
    def _():
        for i in range(1, z_count):
            to_partner(chunk_at(z, i)).start()

    for i in range(z_count):
        with jax.named_scope(f"combine{i}"):
            combine(i)
    with jax.named_scope("drain"):
        drain()
    for i in range(z_count):
        with jax.named_scope(f"finish{i}"):
            finish(i)
    with jax.named_scope("result_x"):
        for k in range(2):
            to_x(jnp.int32(k)).wait_recv()
    out_ref[lines_of(1 - x), :] = xo_recv[...]

    for k in range(3):
        whole = zs_send.at[k]
        remote(whole, whole, rs_s.at[k], xo_r.at[0], x_peer).wait_send()
    remote(xo_send, xo_recv, x_sem.at[4], xo_r.at[0], x_peer).wait_send()


def fits(mesh, units):
    if mesh.shape["tp"] != X or mesh.shape["sp"] != 4 * Y * C:
        return False
    return units % (X * LANES) == 0 and units // (X * LANES) % 4 == 2


def fused(mesh):
    sp_count = mesh.shape["sp"]
    z_count = sp_count // (Y * C)

    def shard(
        query_content,
        query_rotary,
        latents,
        key_rotary,
        latent_gain,
        key_up,
        value_up,
        out_proj,
        residual,
        mixer_gain,
        gate_proj,
        up_proj,
        down_proj,
    ):
        rows = query_content.shape[0]
        per_device, rank = latents.shape
        chunk = Y * C * X * per_device
        heads = key_up.shape[1] // DN
        half = residual.shape[1]
        depth, units = gate_proj.shape
        least, low, high = split_blocks(units // LANES, z_count)
        pad = (least + 2 - least % 2) * LANES
        model = X * half
        share = rows // X
        places = np.arange(z_count * chunk).reshape(z_count, Y, C, rows)
        places = places.transpose(0, 2, 1, 3).reshape(-1)
        cosines, sines = (t.reshape(z_count, chunk, LANES) for t in rotary_tables(places))
        same, paired = (jnp.asarray(t, BF16) for t in turn_matrices())
        vmem = pl.BlockSpec(memory_space=VMEM)
        hbm = pl.BlockSpec(memory_space=pl.ANY)
        dma = pltpu.SemaphoreType.DMA
        scratch = [
            VMEM((per_device, rank + LANES), BF16),
            VMEM((z_count, C, Y, X, per_device, rank + LANES), BF16),
            VMEM((z_count, chunk, LANES), F32),
            VMEM((z_count, chunk, LANES), F32),
            VMEM(out_proj.shape, BF16),
            VMEM((rows, half), BF16),
            VMEM((model, X * pad), BF16),
            VMEM((model, X * pad), BF16),
            VMEM((sp_count, X * pad, LANES), BF16),
            VMEM((chunk, heads * DN), BF16),
            VMEM((chunk, heads * DV), BF16),
            VMEM((chunk, LANES), BF16),
            VMEM((heads, rows, 2 * LANES), BF16),
            VMEM((heads, rows, LANES), F32),
            VMEM((heads, rows, LANES), F32),
            VMEM((heads, rows, DV), F32),
            VMEM((X, rows, heads * DV), BF16),
            VMEM((X, share, half), BF16),
            VMEM((z_count, share, model), BF16),
            VMEM((z_count * share, model), BF16),
            VMEM((z_count * share, X * pad), BF16),
            VMEM((z_count, z_count * share, Y * C * LANES), F32),
            VMEM((share, model), F32),
            VMEM((3, share, model), BF16),
            VMEM((2, share, model), BF16),
            VMEM((2, share, model), BF16),
            VMEM((share, half), BF16),
            VMEM((share, half), BF16),
            dma((8,)),
            *[dma((z_count,)) for _ in range(8)],
            *[dma((z_count, 3)) for _ in range(2)],
            dma((2, 3)),
            dma((z_count, 2, 3)),
            dma((2, 3)),
            dma((z_count, 2, 3)),
            dma((3,)),
            dma((2 + z_count,)),
            dma((5,)),
            *[dma((z_count,)) for _ in range(3)],
            dma((3,)),
            dma((z_count,)),
            dma((2, z_count)),
            dma((z_count,)),
            dma((2,)),
        ]
        return pl.pallas_call(
            functools.partial(layer_kernel, z_count),
            out_shape=jax.ShapeDtypeStruct(residual.shape, residual.dtype),
            in_specs=[vmem] * 10 + [hbm] * 7,
            out_specs=vmem,
            scratch_shapes=scratch,
            compiler_params=pltpu.CompilerParams(
                collective_id=0, has_side_effects=True, vmem_limit_bytes=60 * 1024 * 1024
            ),
        )(
            query_content,
            query_rotary,
            latents,
            key_rotary.T,
            latent_gain[None, :],
            key_up,
            value_up,
            mixer_gain[None, :],
            same,
            paired,
            out_proj,
            residual,
            gate_proj,
            up_proj,
            down_proj,
            cosines,
            sines,
        )

    return jax.shard_map(
        shard,
        mesh=mesh,
        in_specs=(
            P("sp", None),
            P("sp", None),
            P(("sp", "tp"), None),
            P(("sp", "tp"), None),
            P(),
            P(None, "tp"),
            P(None, "tp"),
            P(None, "tp"),
            P("sp", "tp"),
            P(),
            P("sp", "tp"),
            P("sp", "tp"),
            P("tp", "sp"),
        ),
        out_specs=P("sp", "tp"),
        check_vma=False,
    )


def plain(mesh):
    sp_count, tp_count = mesh.shape["sp"], mesh.shape["tp"]
    grouped = Mesh(mesh.devices.reshape(sp_count // 4, 2, 2, tp_count), SP + ("tp",))
    return jax.shard_map(
        shards,
        mesh=grouped,
        in_specs=(
            P(SP, None),
            P(SP, None),
            P(SP + ("tp",), None),
            P(SP + ("tp",), None),
            P(),
            P(None, "tp"),
            P(None, "tp"),
            P(None, "tp"),
            P(SP, "tp"),
            P(),
            P(SP, "tp"),
            P(SP, "tp"),
            P("tp", SP),
        ),
        out_specs=P(SP, "tp"),
        check_vma=False,
    )


def solution(mesh):
    def layer(*arrays):
        build = fused if fits(mesh, arrays[10].shape[1]) else plain
        return build(mesh)(*arrays)

    return layer
```

```python
import functools
import math

import jax
import jax.numpy as jnp
import numpy as np
from jax import lax
from jax.experimental import pallas as pl
from jax.experimental.pallas import tpu as pltpu
from jax.sharding import Mesh, PartitionSpec as P

H = 8
DN = 128
DR = 64
DV = 128
SPAN = 64


epsilon = 1e-06
masked_score = -1e30
SP = ("z", "y", "c")


def norm_round(inputs, scales):
    widened = inputs.astype(jnp.float32)
    factor = lax.rsqrt(jnp.mean(widened * widened, axis=-1, keepdims=True) + epsilon)
    return (widened * factor * scales).astype(jnp.bfloat16)


def rotate(inputs, places):
    dimension = inputs.shape[-1]
    middle = dimension // 2
    inverse = 10000.0 ** (-jnp.arange(0, dimension, 2, dtype=jnp.float32) / dimension)
    angles = places.astype(jnp.float32)[:, None, None] * inverse[None, None, :]
    cosine_table = jnp.cos(angles)
    sine_table = jnp.sin(angles)
    widened = inputs.astype(jnp.float32)
    first_half = widened[..., :middle]
    second_half = widened[..., middle:]
    return jnp.concatenate(
        [
            first_half * cosine_table - second_half * sine_table,
            second_half * cosine_table + first_half * sine_table,
        ],
        axis=-1,
    ).astype(jnp.bfloat16)


def hop(inputs, axis, offset):
    count = lax.axis_size(axis)
    return lax.ppermute(inputs, axis, [(i, (i + offset) % count) for i in range(count)])


def others(inputs, axis):
    return [inputs] + [hop(inputs, axis, d) for d in range(1, lax.axis_size(axis))]


def take(inputs, index, count, dim):
    size = inputs.shape[dim] // count
    return lax.dynamic_slice_in_dim(inputs, index * size, size, dim)


def in_order(blocks, axis, dim):
    count, me = lax.axis_size(axis), lax.axis_index(axis)
    if count == 1:
        return blocks[0]
    if count == 2:
        straight = jnp.concatenate(blocks, axis=dim)
        turned = jnp.concatenate(blocks[::-1], axis=dim)
        return jnp.where(me == 0, straight, turned)
    size = blocks[0].shape[dim]
    shape = list(blocks[0].shape)
    shape[dim] = size * count
    result = jnp.zeros(shape, blocks[0].dtype)
    for d, block in enumerate(blocks):
        place = lax.rem(me - d + count, count) * size
        result = lax.dynamic_update_slice_in_dim(result, block, place, dim)
    return result


def shards(
    query_content,
    query_rotary,
    latents,
    key_rotary,
    latent_gain,
    key_up,
    value_up,
    out_proj,
    residual,
    mixer_gain,
    gate_proj,
    up_proj,
    down_proj,
):
    query_rows = query_content.shape[0]
    tp_count, z_count = lax.axis_size("tp"), lax.axis_size("z")
    sp_index, tp_index, z_index = (
        lax.axis_index(SP),
        lax.axis_index("tp"),
        lax.axis_index("z"),
    )
    rank = latents.shape[1]
    per_device = latents.shape[0]
    heads = H // tp_count

    gathered = jnp.concatenate([latents, key_rotary], axis=1)
    places = (sp_index * tp_count + tp_index) * per_device + jnp.arange(
        per_device, dtype=jnp.int32
    )
    strides = {
        "z": lax.axis_size("y") * lax.axis_size("c") * tp_count * per_device,
        "y": lax.axis_size("c") * tp_count * per_device,
        "c": tp_count * per_device,
        "tp": per_device,
    }
    pieces = []
    for weights in (gate_proj, up_proj, down_proj.T):
        rows, columns = weights.shape
        pieces.append(jnp.swapaxes(weights.reshape(rows, z_count, columns // z_count), 0, 1))
    for axis in ("z", "tp", "y", "c"):
        count, me = lax.axis_size(axis), lax.axis_index(axis)
        gathered = jnp.concatenate(others(gathered, axis), axis=0)
        places = jnp.concatenate(
            [places + (lax.rem(me - d + count, count) - me) * strides[axis] for d in range(count)]
        )
        if axis == "z":
            gathered, pieces = lax.optimization_barrier((gathered, pieces))

    whole = []
    for piece in pieces:
        rows, units = piece.shape[1:]
        blocks = []
        for d in range(z_count):
            block = take(piece, lax.rem(z_index + d, z_count), z_count, 0)
            blocks.append(hop(block, "z", d) if d else block)
        block = in_order(blocks, "z", 0)[:, None]
        block = in_order(others(block, "y"), "y", 1)[:, :, None]
        block = in_order(others(block, "c"), "c", 2)
        whole.append(block.reshape(-1, units))
    gate, up, down = whole

    query_places = sp_index * query_rows + jnp.arange(query_rows, dtype=jnp.int32)
    normed = norm_round(gathered[:, :rank], latent_gain)
    key_turned = rotate(gathered[:, None, rank:], places)[:, 0, :]
    own_rotary = take(query_rotary, tp_index, tp_count, 1)
    own_content = take(query_content, tp_index, tp_count, 1)
    query_turned = rotate(own_rotary.reshape(query_rows, heads, DR), query_places)
    allowed = places[None, :] // SPAN <= query_places[:, None] // SPAN
    score_scale = 1.0 / math.sqrt(DN + DR)
    key_rows = jnp.dot(normed, key_up, preferred_element_type=jnp.float32).astype(jnp.bfloat16)
    value_rows = jnp.dot(normed, value_up, preferred_element_type=jnp.float32).astype(jnp.bfloat16)
    outs = []
    for h in range(heads):
        k = jnp.concatenate([key_rows[:, h * DN : (h + 1) * DN], key_turned], axis=1)
        q = jnp.concatenate(
            [own_content[:, h * DN : (h + 1) * DN], query_turned[:, h, :]], axis=1
        )
        scores = lax.dot_general(
            q, k, (((1,), (1,)), ((), ())), preferred_element_type=jnp.float32
        )
        scores = jnp.where(allowed, scores * score_scale, masked_score)
        highest = jnp.max(scores, axis=-1, keepdims=True)
        weights = jnp.where(allowed, jnp.exp(scores - highest), 0.0)
        weight_sum = jnp.sum(weights, axis=-1, keepdims=True)
        weighted = jnp.dot(
            weights.astype(jnp.bfloat16),
            value_rows[:, h * DV : (h + 1) * DV],
            preferred_element_type=jnp.float32,
        )
        outs.append((weighted / weight_sum).astype(jnp.bfloat16))
    own_heads = jnp.concatenate(outs, axis=1)
    total = residual.astype(jnp.float32)
    for d, block in enumerate(others(own_heads, "tp")):
        part = take(out_proj, lax.rem(tp_index - d + tp_count, tp_count), tp_count, 0)
        total = total + jnp.dot(block, part, preferred_element_type=jnp.float32)
    mixed_rows = total.astype(jnp.bfloat16)

    result = mixed_rows.astype(jnp.float32)
    for d, rows in enumerate(others(mixed_rows, "z")):
        normed_rows = norm_round(in_order(others(rows, "tp"), "tp", 1), mixer_gain)
        hidden = (
            jax.nn.silu(jnp.dot(normed_rows, gate, preferred_element_type=jnp.float32))
            * jnp.dot(normed_rows, up, preferred_element_type=jnp.float32)
        ).astype(jnp.bfloat16)

        def share(index):
            part = take(down, lax.rem(index, tp_count), tp_count, 0)
            return lax.dot_general(
                hidden, part, (((1,), (1,)), ((), ())), preferred_element_type=jnp.float32
            )

        arrived = [
            hop(share(tp_index + e).astype(jnp.bfloat16), "tp", e) for e in range(1, tp_count)
        ]
        sums = share(tp_index)
        for part in arrived:
            sums = sums + part.astype(jnp.float32)
        if d:
            sums = hop(sums.astype(jnp.bfloat16), "z", -d).astype(jnp.float32)
        result = result + sums
    return result.astype(jnp.bfloat16)


Y, C, X = 2, 2, 2
LANES = 128
MESH = pl.DeviceIdType.MESH
VMEM = pltpu.VMEM
F32, BF16 = jnp.float32, jnp.bfloat16


def nearest(z_count):
    return [
        sorted(range(z_count), key=lambda s: (abs(s - z), s if 2 * z < z_count else -s))
        for z in range(z_count)
    ]


def pick(index, values):
    result = jnp.int32(values[0])
    for k in range(1, len(values)):
        result = jnp.where(index == k, jnp.int32(values[k]), result)
    return result


def split_blocks(blocks, z_count):
    least, left = divmod(blocks, z_count)
    return least, left - left // 2, z_count - left // 2


def rotary_tables(positions):
    inverse = np.float32(10000.0) ** (-np.arange(0, DR, 2, dtype=np.float32) / np.float32(DR))
    angles = positions.astype(np.float32)[:, None] * inverse.astype(np.float32)[None, :]
    wide = angles.astype(np.float64)
    repeat = LANES // (DR // 2)
    return (
        np.tile(np.cos(wide).astype(np.float32), (1, repeat)),
        np.tile(np.sin(wide).astype(np.float32), (1, repeat)),
    )


def turn_matrices():
    middle = DR // 2
    turn = np.zeros((DR, DR), np.float32)
    for i in range(middle):
        turn[middle + i, i] = -1.0
        turn[i, middle + i] = 1.0
    copies = LANES // DR
    same = np.concatenate([np.eye(DR, dtype=np.float32)] * copies, axis=1)
    paired = np.kron(np.eye(copies, dtype=np.float32), turn)
    return same, paired


def layer_kernel(
    z_count,
    qc_ref,
    qr_ref,
    lat_ref,
    krt_ref,
    lgain_ref,
    key_up_ref,
    value_up_ref,
    mgain_ref,
    same_ref,
    paired_ref,
    oproj_hbm,
    res_hbm,
    gate_hbm,
    up_hbm,
    down_hbm,
    cos_hbm,
    sin_hbm,
    out_ref,
    lat_own,
    lat_buf,
    cos_buf,
    sin_buf,
    oproj_buf,
    res_buf,
    gate_buf,
    up_buf,
    down_buf,
    key_s,
    value_s,
    turn_s,
    q_s,
    max_s,
    sum_s,
    acc_s,
    ho_buf,
    mix_s,
    tok_buf,
    nrm_s,
    hid_s,
    part_s,
    fin_s,
    zs_send,
    zs_recv,
    pair_recv,
    xo_send,
    xo_recv,
    loc_sem,
    lz_s,
    lz_r,
    ly_s,
    ly_r,
    lx_s,
    lx_r,
    lc_s,
    lc_r,
    wz_s,
    wz_r,
    wy_s,
    wy_r,
    wx_s,
    wx_r,
    wc_s,
    wc_r,
    x_sem,
    tu_s,
    td_s,
    tz_r,
    rs_s,
    ra_r,
    rb_r,
    rc_r,
    xo_r,
):
    sp, x = lax.axis_index("sp"), lax.axis_index("tp")
    z, y, c = sp // (Y * C), (sp // C) % Y, sp % C
    order = nearest(z_count)
    rows = qc_ref.shape[0]
    per_device = lat_ref.shape[0]
    rank = lat_ref.shape[1]
    chunk = Y * C * X * per_device
    heads = key_up_ref.shape[1] // DN
    depth = gate_hbm.shape[0]
    blocks = gate_hbm.shape[1] // LANES
    least, low, high = split_blocks(blocks, z_count)
    main = least * LANES
    half = res_hbm.shape[1]
    pad = gate_buf.shape[1] // X
    share = rows // X
    cut = C * Y * LANES

    def dev(zz, yy, cc, xx):
        return ((zz * Y + yy) * C + cc, xx)

    def has_extra(zz, xx):
        ends = (zz < low) | (zz >= high)
        return jnp.where(ends, 1, 0) + xx == 1

    def offset(zz, xx):
        before = jnp.minimum(zz, low) + jnp.maximum(zz - high, 0)
        return (zz * least + before + xx * (zz - 2 * before)) * LANES

    def remote(src, dst, send, recv, to):
        return pltpu.make_async_remote_copy(
            src_ref=src,
            dst_ref=dst,
            send_sem=send,
            recv_sem=recv,
            device_id=to,
            device_id_type=MESH,
        )

    y_peer, x_peer, c_peer = dev(z, 1 - y, c, x), dev(z, y, c, 1 - x), dev(z, y, 1 - c, x)

    def each_part(zz, action, xx=x):
        @pl.when(has_extra(zz, xx))
        def _():
            action(True)

        @pl.when(jnp.logical_not(has_extra(zz, xx)))
        def _():
            action(False)

    barrier = pltpu.get_barrier_semaphore()
    for peer in (y_peer, x_peer, c_peer):
        pl.semaphore_signal(barrier, inc=1, device_id=peer, device_id_type=MESH)
    for d in range(1, z_count):
        pl.semaphore_signal(
            barrier,
            inc=1,
            device_id=dev(lax.rem(z + d, z_count), y, c, x),
            device_id_type=MESH,
        )
    slot = sp

    def weight_block(m, index, xx, extra):
        start = pl.multiple_of(xx * pad, LANES)
        span = pl.ds(start, main + LANES if extra else main)
        if m < 2:
            buf = (gate_buf, up_buf)[m]
            return buf.at[pl.ds(pl.multiple_of(index * depth, depth), depth), span]
        return down_buf.at[index, span]

    def weight_source(m, zz, extra):
        start = pl.multiple_of(offset(zz, x), LANES)
        size = main + LANES if extra else main
        if m < 2:
            return (gate_hbm, up_hbm)[m].at[:, pl.ds(start, size)]
        return down_hbm.at[pl.ds(start, size)]

    locals_ = [
        (lat_own, lat_buf.at[z, c, y, x], 0),
        (cos_hbm, cos_buf, 1),
        (sin_hbm, sin_buf, 2),
        (oproj_hbm, oproj_buf, 3),
        (res_hbm, res_buf, 4),
    ]

    def local(k):
        src, dst, sem = locals_[k]
        return pltpu.make_async_copy(src, dst, loc_sem.at[sem])

    def own_weight(m, extra):
        return pltpu.make_async_copy(
            weight_source(m, z, extra),
            weight_block(m, slot, x, extra),
            loc_sem.at[5 + m],
        )

    lat_own[:, :rank] = lat_ref[...]
    lat_own[:, rank:] = lax.dot_general(
        krt_ref[...], same_ref[...], (((0,), (0,)), ((), ())), preferred_element_type=F32
    ).astype(BF16)
    for k in range(1, len(locals_)):
        local(k).start()
    for m in range(3):
        each_part(z, lambda e: own_weight(m, e).start())

    for xx in range(X):

        @pl.when(jnp.logical_not(has_extra(z, xx)))
        def _():
            tail = slice(xx * pad + main, (xx + 1) * pad)
            gate_buf[:, tail] = jnp.zeros((gate_buf.shape[0], pad - main), BF16)
            up_buf[:, tail] = jnp.zeros((up_buf.shape[0], pad - main), BF16)
            down_buf[:, tail, :] = jnp.zeros((down_buf.shape[0], pad - main, LANES), BF16)

    with jax.named_scope('entry'):
        pl.semaphore_wait(barrier, 3 + z_count - 1)

    def lat_z(source, target):
        return remote(
            lat_own,
            lat_buf.at[source, c, y, x],
            lz_s.at[target],
            lz_r.at[source],
            dev(target, y, c, x),
        )

    def lat_y(zz, yy):
        block = lat_buf.at[zz, c, yy, x]
        return remote(block, block, ly_s.at[zz], ly_r.at[zz], y_peer)

    def lat_x(zz, xx):
        block = lat_buf.at[zz, c, :, xx]
        return remote(block, block, lx_s.at[zz], lx_r.at[zz], x_peer)

    def lat_c(zz, cc):
        block = lat_buf.at[zz, cc]
        return remote(block, block, lc_s.at[zz], lc_r.at[zz], c_peer)

    local(0).start()
    local(0).wait()
    lat_y(z, y).start()
    for d in range(1, z_count):

        @pl.when(z + d < z_count)
        def _():
            lat_z(z, z + d).start()

    def weight_z(m, source, target, extra, index):
        return remote(
            weight_source(m, target, extra),
            weight_block(m, index, x, extra),
            wz_s.at[target, m],
            wz_r.at[source, m],
            dev(target, y, c, x),
        )

    def at(s):
        return pick(z, [o[s] for o in order])

    def send_z(m, s):
        each_part(at(s), lambda e: weight_z(m, z, at(s), e, slot).start())

    for m in range(2):
        for s in range(1, z_count):
            send_z(m, s)

    def block_of(zz, yy, cc):
        return (zz * Y + yy) * C + cc

    def weight_y(m, zz, yy, xx, hop, extra):
        block = weight_block(m, block_of(zz, yy, c), xx, extra)
        return remote(block, block, wy_s.at[hop, m], wy_r.at[zz, hop, m], y_peer)

    def weight_x(m, zz, yy, xx, hop, extra):
        block = weight_block(m, block_of(zz, yy, c), xx, extra)
        return remote(block, block, wx_s.at[hop, m], wx_r.at[zz, hop, m], x_peer)

    def weight_c(m, zz, yy, xx, cc, extra):
        block = weight_block(m, block_of(zz, yy, cc), xx, extra)
        arrival = wc_r.at[m] if m < 2 else wc_r.at[2 + zz]
        return remote(block, block, wc_s.at[m], arrival, c_peer)

    def y_first(m, s):
        return (False, s % 2 == 1, s % 2 == 1)[m]

    def to_core(m, zz, yy, xx):
        each_part(z, lambda e: weight_c(m, zz, yy, xx, c, e).start(), xx)

    def relay_own(m, s):
        zz = at(s)
        if s:
            each_part(z, lambda e: weight_z(m, zz, z, e, block_of(zz, y, c)).wait_recv())
        else:
            each_part(z, lambda e: own_weight(m, e).wait())
        each_part(z, lambda e: weight_y(m, zz, y, x, 0, e).start())
        to_core(m, zz, y, x)

    def relay_own_x(m, s):
        each_part(z, lambda e: weight_x(m, at(s), y, x, 0, e).start())

    def relay_second(m, s):
        zz = at(s)
        if y_first(m, s):
            each_part(z, lambda e: weight_y(m, zz, 1 - y, x, 0, e).wait_recv())
            each_part(z, lambda e: weight_x(m, zz, 1 - y, x, 1, e).start())
            to_core(m, zz, 1 - y, x)
        else:
            each_part(z, lambda e: weight_x(m, zz, y, 1 - x, 0, e).wait_recv(), 1 - x)
            each_part(z, lambda e: weight_y(m, zz, y, 1 - x, 1, e).start(), 1 - x)
            to_core(m, zz, y, 1 - x)

    def relay_last(m, s):
        zz = at(s)
        if y_first(m, s):
            each_part(z, lambda e: weight_x(m, zz, y, 1 - x, 0, e).wait_recv(), 1 - x)
            to_core(m, zz, y, 1 - x)
            each_part(z, lambda e: weight_x(m, zz, 1 - y, 1 - x, 1, e).wait_recv(), 1 - x)
        else:
            each_part(z, lambda e: weight_y(m, zz, 1 - y, x, 0, e).wait_recv())
            to_core(m, zz, 1 - y, x)
            each_part(z, lambda e: weight_y(m, zz, 1 - y, 1 - x, 1, e).wait_recv(), 1 - x)
        to_core(m, zz, 1 - y, 1 - x)

    pieces = [(0, 0), (1, 0)]
    pieces += [(0, s) for s in range(1, z_count)] + [(1, s) for s in range(1, z_count)]
    pieces += [(2, s) for s in range(z_count)]

    def relay(name, *steps):
        for kind, *ks in steps:
            for k in ks:
                with jax.named_scope(f"{name}_{kind}{k}"):
                    if kind in "ap":
                        relay_own(*pieces[k])
                    if kind in "aq":
                        relay_own_x(*pieces[k])
                    if kind == "b":
                        relay_second(*pieces[k])
                    if kind == "c":
                        relay_last(*pieces[k])

    relay('r0', ('a', 0))
    with jax.named_scope("lat_y_own"):
        lat_y(z, 1 - y).wait_recv()
        lat_x(z, x).start()

    def lower(action):
        for d in range(1, z_count):

            @pl.when(z >= d)
            def _():
                action(z - d)

    def y_step(zz):
        lat_z(zz, z).wait_recv()
        lat_y(zz, y).start()

    def x_step(zz):
        lat_y(zz, 1 - y).wait_recv()
        lat_x(zz, x).start()

    def c_step(zz):
        lat_x(zz, 1 - x).wait_recv()
        lat_c(zz, c).start()

    with jax.named_scope("lat_z"):
        lower(y_step)
    relay('r0', ('p', 1))
    with jax.named_scope("lat_x_own"):
        lat_x(z, 1 - x).wait_recv()
        lat_c(z, c).start()

    local(1).wait()
    local(2).wait()
    q_start = pl.multiple_of((c * Y + y) * rows, rows)
    cos_q = cos_buf[z, pl.ds(q_start, rows), :]
    sin_q = sin_buf[z, pl.ds(q_start, rows), :]
    lane = lax.broadcasted_iota(jnp.int32, (rows, LANES), 1)
    for pair in range(heads * DR // LANES):
        start = pl.multiple_of(x * heads * DR + pair * LANES, LANES)
        part = qr_ref[:, pl.ds(start, LANES)]
        swapped = jnp.dot(part, paired_ref[...], preferred_element_type=F32)
        turned = (part.astype(F32) * cos_q + swapped * sin_q).astype(BF16)
        for k in range(LANES // DR):
            h = pair * (LANES // DR) + k
            keep = (lane >= k * DR) & (lane < (k + 1) * DR)
            q_s[h, :, LANES:] = jnp.where(keep, turned, jnp.zeros_like(turned))
    for h in range(heads):
        start = pl.multiple_of(x * heads * DN + h * DN, DN)
        q_s[h, :, :LANES] = qc_ref[:, pl.ds(start, DN)]

    scale = 1.0 / math.sqrt(DN + DR)
    max_s[...] = jnp.full(max_s.shape, masked_score, F32)
    sum_s[...] = jnp.zeros(sum_s.shape, F32)
    acc_s[...] = jnp.zeros(acc_s.shape, F32)
    key_id = lax.broadcasted_iota(jnp.int32, (rows, chunk), 1)
    per_c, per_y = Y * X * per_device, X * per_device
    c_id = key_id // per_c
    y_id = (key_id // per_y) % Y
    key_place = y_id * C * per_y + c_id * per_y + key_id % per_y
    query_place = (y * C + c) * per_y + lax.broadcasted_iota(jnp.int32, (rows, chunk), 0)

    def attend(d):
        zz = z - d
        lat_c(zz, 1 - c).wait_recv()
        both = lat_buf[zz].reshape(chunk, rank + LANES)
        wide = both[:, :rank].astype(F32)
        factor = lax.rsqrt(jnp.mean(wide * wide, axis=-1, keepdims=True) + epsilon)
        normed = (wide * factor * lgain_ref[...]).astype(BF16)
        key_s[...] = jnp.dot(normed, key_up_ref[...], preferred_element_type=F32).astype(BF16)
        value_s[...] = jnp.dot(normed, value_up_ref[...], preferred_element_type=F32).astype(BF16)
        rot = both[:, rank:]
        swapped = jnp.dot(rot, paired_ref[...], preferred_element_type=F32)
        turn_s[...] = (rot.astype(F32) * cos_buf[zz] + swapped * sin_buf[zz]).astype(BF16)
        allowed = (key_place - d * chunk) // SPAN <= query_place // SPAN
        for h in range(heads):
            k = jnp.concatenate([key_s[:, h * DN : (h + 1) * DN], turn_s[...]], axis=1)
            scores = lax.dot_general(
                q_s[h], k, (((1,), (1,)), ((), ())), preferred_element_type=F32
            )
            if d:
                scores = scores * scale
            else:
                scores = jnp.where(allowed, scores * scale, masked_score)
            before = max_s[h, :, :1]
            peak = jnp.maximum(before, jnp.max(scores, axis=-1, keepdims=True))
            weights = jnp.exp(scores - peak)
            fade = jnp.exp(before - peak)
            total = sum_s[h, :, :1] * fade + jnp.sum(weights, axis=-1, keepdims=True)
            gained = jnp.dot(
                weights.astype(BF16),
                value_s[:, h * DV : (h + 1) * DV],
                preferred_element_type=F32,
            )
            acc_s[h] = acc_s[h] * fade + gained
            max_s[h] = jnp.broadcast_to(peak, max_s.shape[1:])
            sum_s[h] = jnp.broadcast_to(total, sum_s.shape[1:])

    with jax.named_scope("lat_y"):
        lower(x_step)
    relay("r1", ("b", 0), ("q", 1), ("p", 8))
    with jax.named_scope("attend0"):
        attend(0)
    with jax.named_scope("lat_x"):
        lower(c_step)
    relay("r2", ("a", 2))
    for d in range(1, z_count):

        @pl.when(z >= d)
        def _():
            with jax.named_scope(f"attend{d}"):
                attend(d)

        if d < z_count - 1:
            if d == 2:
                relay("r3", ("b", 1))

    for h in range(heads):
        ho_buf[x, :, h * DV : (h + 1) * DV] = (acc_s[h] / sum_s[h]).astype(BF16)

    def heads_out(xx):
        return remote(ho_buf.at[xx], ho_buf.at[xx], x_sem.at[0], x_sem.at[1], x_peer)

    heads_out(x).start()
    relay("r5", ("a", 3), ("p", 4))

    local(3).wait()
    local(4).wait()
    width = heads * DV
    with jax.named_scope("heads_wait"):
        heads_out(1 - x).wait_recv()
    total = res_buf[...].astype(F32)
    for k in range(X):
        total = total + jnp.dot(
            ho_buf[k], oproj_buf[k * width : (k + 1) * width, :], preferred_element_type=F32
        )
    mix_s[...] = total.astype(BF16).reshape(X, share, half)

    def features(xx):
        return pl.ds(pl.multiple_of(xx * half, LANES), half)

    def tok_x(to):
        return remote(
            mix_s.at[to],
            tok_buf.at[z, :, features(1 - to)],
            x_sem.at[2],
            x_sem.at[3],
            x_peer,
        )

    tok_x(1 - x).start()
    tok_buf[z, :, features(x)] = mix_s[x]
    outer = (z == 0) | (z == z_count - 1)
    send_z(2, 1)

    @pl.when(outer)
    def _():
        for s in range(2, z_count):
            send_z(2, s)

    relay("r6", ("b", 2), ("q", 4), ("b", 3), ("a", 5), ("c", 0, 1))
    with jax.named_scope("tok_x"):
        tok_x(x).wait_recv()

    token_parts = 2
    lines_part = share // token_parts

    def tok_z(zz, to, sem, part):
        block = tok_buf.at[zz, pl.ds(part * lines_part, lines_part)]
        return remote(block, block, sem.at[zz, part], tz_r.at[zz, part], dev(to, y, c, x))

    def goes_up(zz):
        return (zz <= z) & (z + 1 < z_count)

    def goes_down(zz):
        return (zz >= z) & (z > 0)

    def forward(zz, part):
        @pl.when(goes_up(zz))
        def _():
            tok_z(zz, z + 1, tu_s, part).start()

        @pl.when(goes_down(zz))
        def _():
            tok_z(zz, z - 1, td_s, part).start()

    def relay_tokens(zz, name):
        with jax.named_scope(f"rt_{name}"):
            for part in range(token_parts):
                tok_z(zz, z, tu_s, part).wait_recv()
                forward(zz, part)

    def normalize(s):
        zz = at(s)
        wide = tok_buf[zz].astype(F32)
        factor = lax.rsqrt(jnp.mean(wide * wide, axis=-1, keepdims=True) + epsilon)
        lines = pl.ds(pl.multiple_of(zz * share, share), share)
        nrm_s[lines, :] = (wide * factor * mgain_ref[...]).astype(BF16)

    for part in range(token_parts):
        forward(z, part)
    relay("r7", ("a", 6), ("b", 4), ("a", 7), ("c", 2))
    normalize(0)
    inner = jnp.logical_not(outer)

    @pl.when(inner)
    def _():
        relay_tokens(z - 1, "below")

    relay("r7", ("b", 5))

    @pl.when(inner)
    def _():
        relay_tokens(z + 1, "above")
        for s in range(2, z_count):
            send_z(2, s)

    relay("r8", ("b", 6), ("q", 8), ("p", 9))

    @pl.when(inner)
    def _():
        relay_tokens(at(3), "far")

    relay("r8", ("b", 7), ("c", 3), ("q", 9))
    @pl.when(inner)
    def _():
        relay("r9", ("c", 4, 5), ("a", 10), ("c", 6), ("a", 11), ("c", 7), ("b", 8))

    @pl.when(outer)
    def _():
        relay("r9", ("c", 4, 5, 6, 7), ("a", 10), ("b", 8), ("a", 11))
        for s in range(1, z_count):
            relay_tokens(at(s), f"{s}")

    for s in range(1, z_count):
        normalize(s)

    both_widths = 2 * main + LANES

    def wait_core(m):
        lines = z_count * Y * X // 2 * depth
        whole = (gate_buf, up_buf)[m].at[pl.ds(0, lines), pl.ds(0, both_widths)]
        remote(whole, whole, wc_s.at[m], wc_r.at[m], c_peer).wait_recv()

    def wait_down(zz):
        whole = down_buf.at[pl.ds(0, X * Y // 2), pl.ds(0, both_widths)]
        remote(whole, whole, wc_s.at[2], wc_r.at[2 + zz], c_peer).wait_recv()

    with jax.named_scope("wait_gu"):
        for m in range(2):
            wait_core(m)

    wide_tile = 2 * LANES

    def hidden(n, carry):
        lanes = pl.ds(pl.multiple_of(n * wide_tile, wide_tile), wide_tile)
        g = jnp.dot(nrm_s[...], gate_buf[:, lanes], preferred_element_type=F32)
        u = jnp.dot(nrm_s[...], up_buf[:, lanes], preferred_element_type=F32)
        hid_s[:, lanes] = (g / (1.0 + jnp.exp(-g)) * u).astype(BF16)
        return carry

    tiles = X * pad // wide_tile
    with jax.named_scope("hidden_a"):
        lax.fori_loop(0, tiles // 2, hidden, 0)
    relay("r13", ("b", 9))

    @pl.when(inner)
    def _():
        relay("r13", ("b", 10))

    with jax.named_scope("hidden_b"):
        lax.fori_loop(tiles // 2, tiles, hidden, 0)

    def columns(zz):
        return pl.ds(pl.multiple_of(zz * cut, cut), cut)

    partner = z + 1 - 2 * (z % 2)
    across = [2 * (1 - z // 2) + j for j in range(2)]

    def to_partner(zc):
        return remote(
            zs_send.at[0, :, columns(zc)],
            zs_recv.at[0, :, columns(zc)],
            rs_s.at[0],
            ra_r.at[zc],
            dev(partner, y, c, x),
        )

    def to_pair(j, zc):
        return remote(
            zs_send.at[1 + j, :, columns(zc)],
            pair_recv.at[j, :, columns(zc)],
            rs_s.at[1 + j],
            rb_r.at[j, zc],
            dev(partner, y, c, x),
        )

    def to_across(j, zc):
        return remote(
            zs_send.at[1 + j, :, columns(zc)],
            zs_recv.at[1, :, columns(zc)],
            rs_s.at[1 + j],
            rc_r.at[zc],
            dev(across[j], y, c, x),
        )

    def lines_of(zz):
        return pl.ds(pl.multiple_of(zz * share, share), share)

    early = (((0, 2, 3, 1), (1, 2, 3, 0), (2, 3, 1, 0), (3, 2, 1, 0)),
             ((0, 1, 2, 3), (1, 0, 2, 3), (2, 1, 0, 3), (3, 1, 0, 2)))

    def chunk_at(zz, i):
        return jnp.where(
            x == 0,
            pick(zz, [early[0][k][i] for k in range(z_count)]),
            pick(zz, [early[1][k][i] for k in range(z_count)]),
        )

    def mix(i):
        zc = chunk_at(z, i)
        for n in range(cut // wide_tile):
            first = zc * (Y * C) + 2 * n
            w = jnp.concatenate([down_buf[first], down_buf[first + 1]], axis=1)
            lanes = pl.ds(n * wide_tile, wide_tile)
            part_s[zc, :, lanes] = jnp.dot(hid_s[...], w, preferred_element_type=F32)
        @pl.when(outer)
        def _():
            for j in range(2):
                mine = part_s[zc, lines_of(across[j]), :]
                zs_send[1 + j, :, columns(zc)] = mine.astype(BF16)
                to_pair(j, zc).start()

        zs_send[0, :, columns(zc)] = part_s[zc, lines_of(partner), :].astype(BF16)

        if i == 0:
            to_partner(zc).start()
        else:

            @pl.when(inner)
            def _():
                to_partner(zc).start()

        fin_s[:, columns(zc)] = part_s[zc, lines_of(z), :] + tok_buf[z, :, columns(zc)].astype(F32)

    def combine(i):
        zc = chunk_at(jnp.where(z < 2, 0, z_count - 1), i)

        @pl.when(jnp.logical_not(outer))
        def _():
            for j in range(2):
                to_pair(j, zc).wait_recv()
                both = part_s[zc, lines_of(across[j]), :] + pair_recv[j, :, columns(zc)].astype(F32)
                zs_send[1 + j, :, columns(zc)] = both.astype(BF16)
                to_across(j, zc).start()

    def to_x(zc):
        lanes = pl.ds(pl.multiple_of(zc % 2 * cut, cut), cut)
        return remote(
            xo_send.at[:, lanes], xo_recv.at[:, lanes], x_sem.at[4], xo_r.at[zc % 2], x_peer
        )

    def finish(i):
        zc = chunk_at(jnp.where((z < 2) == outer, z_count - 1, 0), i)
        lanes = pl.ds(pl.multiple_of(zc % 2 * cut, cut), cut)
        to_partner(zc).wait_recv()
        to_across(0, zc).wait_recv()
        result = fin_s[:, columns(zc)]
        for k in range(2):
            result = result + zs_recv[k, :, columns(zc)].astype(F32)

        @pl.when(zc // 2 == x)
        def _():
            out_ref[lines_of(x), lanes] = result.astype(BF16)

        @pl.when(zc // 2 != x)
        def _():
            xo_send[:, lanes] = result.astype(BF16)
            to_x(zc).start()

    def sent(m, sem, count, xx):
        def wait(e):
            size = main + LANES if e else main
            if m < 2:
                ref = (gate_buf, up_buf)[m].at[pl.ds(0, count * depth), pl.ds(0, size)]
            else:
                ref = down_buf.at[pl.ds(0, count), pl.ds(0, size)]
            remote(ref, ref, sem, wz_r.at[0, 0], x_peer).wait_send()

        if count:
            each_part(z, wait, xx)

    def sent_core(m):
        count = z_count * Y * X // 2
        if m < 2:
            ref = (gate_buf, up_buf)[m].at[pl.ds(0, count * depth), pl.ds(0, both_widths)]
        else:
            ref = down_buf.at[pl.ds(0, count), pl.ds(0, both_widths)]
        remote(ref, ref, wc_s.at[m], wz_r.at[0, 0], x_peer).wait_send()

    def drain():
        tok_x(1 - x).wait_send()
        heads_out(x).wait_send()
        lat_y(z, y).wait_send()
        lat_x(z, x).wait_send()
        lat_c(z, c).wait_send()
        for d in range(1, z_count):

            @pl.when(z + d < z_count)
            def _():
                lat_z(z, z + d).wait_send()

        def lat_done(zz):
            lat_y(zz, y).wait_send()
            lat_x(zz, x).wait_send()
            lat_c(zz, c).wait_send()

        lower(lat_done)
        for m in range(3):
            second_x = sum(y_first(m, s) for s in range(z_count))
            sent(m, wx_s.at[0, m], z_count, x)
            sent(m, wx_s.at[1, m], second_x, x)
            sent(m, wy_s.at[0, m], z_count, x)
            sent(m, wy_s.at[1, m], z_count - second_x, 1 - x)
            sent_core(m)
            for s in range(1, z_count):
                each_part(at(s), lambda e: weight_z(m, z, at(s), e, slot).wait_send())
        for s in range(z_count):
            zz = at(s)

            @pl.when(goes_up(zz))
            def _():
                for part in range(token_parts):
                    tok_z(zz, z + 1, tu_s, part).wait_send()

            @pl.when(goes_down(zz))
            def _():
                for part in range(token_parts):
                    tok_z(zz, z - 1, td_s, part).wait_send()

    relay("r13", ("c", 8))
    for i in range(z_count):
        if i == 1:

            @pl.when(outer)
            def _():
                relay("r14", ("b", 10))

            relay("r14", ("b", 11), ("c", 9, 10))
        if i == 2:
            relay("r15", ("c", 11))
        with jax.named_scope(f"wait_d{i}"):
            wait_down(chunk_at(z, i))
        with jax.named_scope(f"mix{i}"):
            mix(i)

    @pl.when(outer)
    def _():
        for i in range(1, z_count):
            to_partner(chunk_at(z, i)).start()

    for i in range(z_count):
        with jax.named_scope(f"combine{i}"):
            combine(i)
    with jax.named_scope("drain"):
        drain()
    for i in range(z_count):
        with jax.named_scope(f"finish{i}"):
            finish(i)
    with jax.named_scope("result_x"):
        for k in range(2):
            to_x(jnp.int32(k)).wait_recv()
    out_ref[lines_of(1 - x), :] = xo_recv[...]

    for k in range(3):
        whole = zs_send.at[k]
        remote(whole, whole, rs_s.at[k], xo_r.at[0], x_peer).wait_send()
    remote(xo_send, xo_recv, x_sem.at[4], xo_r.at[0], x_peer).wait_send()


def fits(mesh, units):
    if mesh.shape["tp"] != X or mesh.shape["sp"] != 4 * Y * C:
        return False
    return units % (X * LANES) == 0 and units // (X * LANES) % 4 == 2


def fused(mesh):
    sp_count = mesh.shape["sp"]
    z_count = sp_count // (Y * C)

    def shard(
        query_content,
        query_rotary,
        latents,
        key_rotary,
        latent_gain,
        key_up,
        value_up,
        out_proj,
        residual,
        mixer_gain,
        gate_proj,
        up_proj,
        down_proj,
    ):
        rows = query_content.shape[0]
        per_device, rank = latents.shape
        chunk = Y * C * X * per_device
        heads = key_up.shape[1] // DN
        half = residual.shape[1]
        depth, units = gate_proj.shape
        least, low, high = split_blocks(units // LANES, z_count)
        pad = (least + 2 - least % 2) * LANES
        model = X * half
        share = rows // X
        places = np.arange(z_count * chunk).reshape(z_count, Y, C, rows)
        places = places.transpose(0, 2, 1, 3).reshape(-1)
        cosines, sines = (t.reshape(z_count, chunk, LANES) for t in rotary_tables(places))
        same, paired = (jnp.asarray(t, BF16) for t in turn_matrices())
        vmem = pl.BlockSpec(memory_space=VMEM)
        hbm = pl.BlockSpec(memory_space=pl.ANY)
        dma = pltpu.SemaphoreType.DMA
        scratch = [
            VMEM((per_device, rank + LANES), BF16),
            VMEM((z_count, C, Y, X, per_device, rank + LANES), BF16),
            VMEM((z_count, chunk, LANES), F32),
            VMEM((z_count, chunk, LANES), F32),
            VMEM(out_proj.shape, BF16),
            VMEM((rows, half), BF16),
            VMEM((model, X * pad), BF16),
            VMEM((model, X * pad), BF16),
            VMEM((sp_count, X * pad, LANES), BF16),
            VMEM((chunk, heads * DN), BF16),
            VMEM((chunk, heads * DV), BF16),
            VMEM((chunk, LANES), BF16),
            VMEM((heads, rows, 2 * LANES), BF16),
            VMEM((heads, rows, LANES), F32),
            VMEM((heads, rows, LANES), F32),
            VMEM((heads, rows, DV), F32),
            VMEM((X, rows, heads * DV), BF16),
            VMEM((X, share, half), BF16),
            VMEM((z_count, share, model), BF16),
            VMEM((z_count * share, model), BF16),
            VMEM((z_count * share, X * pad), BF16),
            VMEM((z_count, z_count * share, Y * C * LANES), F32),
            VMEM((share, model), F32),
            VMEM((3, share, model), BF16),
            VMEM((2, share, model), BF16),
            VMEM((2, share, model), BF16),
            VMEM((share, half), BF16),
            VMEM((share, half), BF16),
            dma((8,)),
            *[dma((z_count,)) for _ in range(8)],
            *[dma((z_count, 3)) for _ in range(2)],
            dma((2, 3)),
            dma((z_count, 2, 3)),
            dma((2, 3)),
            dma((z_count, 2, 3)),
            dma((3,)),
            dma((2 + z_count,)),
            dma((5,)),
            *[dma((z_count, 2)) for _ in range(3)],
            dma((3,)),
            dma((z_count,)),
            dma((2, z_count)),
            dma((z_count,)),
            dma((2,)),
        ]
        return pl.pallas_call(
            functools.partial(layer_kernel, z_count),
            out_shape=jax.ShapeDtypeStruct(residual.shape, residual.dtype),
            in_specs=[vmem] * 10 + [hbm] * 7,
            out_specs=vmem,
            scratch_shapes=scratch,
            compiler_params=pltpu.CompilerParams(
                collective_id=0, has_side_effects=True, vmem_limit_bytes=60 * 1024 * 1024
            ),
        )(
            query_content,
            query_rotary,
            latents,
            key_rotary.T,
            latent_gain[None, :],
            key_up,
            value_up,
            mixer_gain[None, :],
            same,
            paired,
            out_proj,
            residual,
            gate_proj,
            up_proj,
            down_proj,
            cosines,
            sines,
        )

    return jax.shard_map(
        shard,
        mesh=mesh,
        in_specs=(
            P("sp", None),
            P("sp", None),
            P(("sp", "tp"), None),
            P(("sp", "tp"), None),
            P(),
            P(None, "tp"),
            P(None, "tp"),
            P(None, "tp"),
            P("sp", "tp"),
            P(),
            P("sp", "tp"),
            P("sp", "tp"),
            P("tp", "sp"),
        ),
        out_specs=P("sp", "tp"),
        check_vma=False,
    )


def plain(mesh):
    sp_count, tp_count = mesh.shape["sp"], mesh.shape["tp"]
    grouped = Mesh(mesh.devices.reshape(sp_count // 4, 2, 2, tp_count), SP + ("tp",))
    return jax.shard_map(
        shards,
        mesh=grouped,
        in_specs=(
            P(SP, None),
            P(SP, None),
            P(SP + ("tp",), None),
            P(SP + ("tp",), None),
            P(),
            P(None, "tp"),
            P(None, "tp"),
            P(None, "tp"),
            P(SP, "tp"),
            P(),
            P(SP, "tp"),
            P(SP, "tp"),
            P("tp", SP),
        ),
        out_specs=P(SP, "tp"),
        check_vma=False,
    )


def solution(mesh):
    def layer(*arrays):
        build = fused if fits(mesh, arrays[10].shape[1]) else plain
        return build(mesh)(*arrays)

    return layer
```
